256 devices in a mesh: sp: 64 (over z, x, core), tp: 4 (over y).
Axes of the slice: x: 4, y: 4, z: 8, core: 2. Of those that a mesh axis runs over, the one named last changes fastest.
Arguments:
- queries: bfloat16 [8192, 2048], P('sp', 'tp'), may hold values from -6 to 6
- keys: bfloat16 [8192, 512], P('sp', 'tp'), may hold values from -6 to 6
- values: bfloat16 [8192, 512], P('sp', 'tp'), may hold values from -6 to 6
- break_bias: float32 [16], P('tp'), as said below
- residual: bfloat16 [8192, 4096], P(('sp', 'tp')), may hold values from -6 to 6
- w_out: bfloat16 [2048, 4096], P('tp'), may hold values from -0.125 to 0.125
- ffn_gain: float32 [4096], replicated, may hold values from 0.1 to 1.9
- pick_ids: int32 [8192, 2], P('sp'), may hold values from 0 to 63, as said below
- pair_logit: float32 [8192], P('sp'), may hold values from -8 to 8
- w_gate: bfloat16 [64, 4096, 1024], P('sp', None, 'tp'), may hold values from -0.09375 to 0.09375
- w_up: bfloat16 [64, 4096, 1024], P('sp', None, 'tp'), may hold values from -0.09375 to 0.09375
- w_down: bfloat16 [64, 1024, 4096], P('sp', 'tp'), may hold values from -0.1875 to 0.1875
- out_gain: float32 [4096], replicated, may hold values from 0.1 to 1.9
Outputs:
- new_stream: bfloat16 [8192, 4096], P(('sp', 'tp'))
The draws below stay inside these ranges and needn't reach their ends.
Inputs may be any that keep to these rules, and one draw needn't show every extreme that they name: `break_bias`: the logarithm of a break rate per position: between ln(0.02 / 8192) and ln(8 / 128). `pick_ids`: A row's 2 experts differ and lie in one group of 16 consecutive experts. In each aligned block of 32 rows no expert is named more than 2 times, and some expert exactly 2 times.
All inputs are finite; a program needn't handle non-finite values.
Results may differ from the reference program's by a relative error of at most 0.017.
Values may be sent and summed in bfloat16 or wider, within the bound.
A program may use at most 64 MiB of HBM per device.

```python
import jax
import jax.numpy as jnp
from jax import lax

D = 4096
HEAD = 128
HEADS = 16
KV_HEADS = 4
FF = 1024
GROUPS = 4
TOP = 2
TOK_DEV = 128
TOKENS = 8192
EXPERTS = 64
PER = 16
ROWS_DEV = 32
CAP = 2
N_SP = 64
N_TP = 4


def draw_break_bias(key, part):
    key_kind, key_fast, key_slow = jax.random.split(key, 3)
    fast_share = 0.5
    fast = jax.random.uniform(key_kind, (HEADS,), jnp.float32) < fast_share
    fast_rate = jax.random.uniform(key_fast, (HEADS,), jnp.float32, 3.0, 8.0) / TOK_DEV
    slow_rate = jax.random.uniform(key_slow, (HEADS,), jnp.float32, 0.02, 0.2) / TOKENS
    return jnp.log(jnp.where(fast, fast_rate, slow_rate)).astype(jnp.float32)


def pick_block(key):
    pairs = EXPERTS * CAP // 2
    half_group = PER // 2
    key_label, key_force, key_rank, key_rows = jax.random.split(key, 4)
    rounds = GROUPS * CAP
    labels = jax.vmap(lambda sub_key: jax.random.permutation(sub_key, PER))(jax.random.split(key_label, rounds))
    index = jnp.arange(pairs, dtype=jnp.int32)
    round_id = index // half_group
    inside = index % half_group
    group_id = round_id // CAP
    leading = group_id * PER + labels[round_id, 2 * inside]
    trailing = group_id * PER + labels[round_id, 2 * inside + 1]
    forced = jax.random.randint(key_force, (), 0, EXPERTS)
    hit = ((leading == forced) | (trailing == forced)).astype(jnp.int32)
    ranks = jax.random.permutation(key_rank, pairs).astype(jnp.int32)
    chosen = jnp.argsort(ranks - pairs * hit, stable=True)[:ROWS_DEV]
    chosen = chosen[jax.random.permutation(key_rows, ROWS_DEV)]
    return jnp.stack([leading[chosen], trailing[chosen]], axis=1).astype(jnp.int32)


def draw_pick_ids(key, part):
    blocks = TOKENS // ROWS_DEV
    return jax.vmap(pick_block)(jax.random.split(key, blocks)).reshape(TOKENS, TOP).astype(jnp.int32)


def block_levels(key, shape, cuts, least, largest):
    loudness, own = 1.0, jax.random.fold_in(key, 6)
    for axis_at, blocks in cuts:
        heights = jnp.exp(jax.random.uniform(jax.random.fold_in(own, axis_at), (blocks,), jnp.float32, least / len(cuts), largest / len(cuts)))
        loudness = loudness * jnp.repeat(heights, shape[axis_at] // blocks).reshape([-1 if axis == axis_at else 1 for axis in range(len(shape))])
    return loudness


def centred(rng, dims, scale, most, cuts=(), kind=jnp.bfloat16):
    factor_of = block_levels(rng, dims, cuts, -0.22, 0.18) if cuts else 1.0
    drawn = jax.random.normal(rng, dims, jnp.float32) * scale * factor_of
    return jnp.minimum(jnp.maximum(drawn, -most), most).astype(kind)


def setup_inputs(seed: int = 0) -> dict:
    key_list = jax.random.split(jax.random.key(seed), 14)
    queries = centred(key_list[0], (TOKENS, HEADS * HEAD), 1.0, 6.0, ((0, 64), (1, 4)))
    keys = centred(key_list[1], (TOKENS, KV_HEADS * HEAD), 1.0, 6.0, ((0, 64), (1, 4)))
    values = centred(key_list[2], (TOKENS, KV_HEADS * HEAD), 1.0, 6.0, ((0, 64), (1, 4)))
    break_bias = draw_break_bias(jax.random.fold_in(key_list[13], 71), 0)
    residual = centred(key_list[4], (TOKENS, D), 1.0, 6.0, ((0, 256),))
    w_out = centred(key_list[5], (HEADS * HEAD, D), (HEADS * HEAD) ** -0.5, 0.125, ((0, 4),))
    ffn_gain = jnp.clip(1.0 + 0.18 * jax.random.normal(key_list[6], (D,), jnp.float32), 0.1, 1.9)
    pick_ids = draw_pick_ids(jax.random.fold_in(key_list[13], 71), 0)
    pair_logit = centred(key_list[8], (TOKENS,), 1.5, 8.0, ((0, 64),), jnp.float32)
    w_gate = centred(key_list[9], (EXPERTS, D, FF), D ** -0.5, 0.09375, ((0, 64), (2, 4)))
    w_up = centred(key_list[10], (EXPERTS, D, FF), D ** -0.5, 0.09375, ((0, 64), (2, 4)))
    w_down = centred(key_list[11], (EXPERTS, FF, D), FF ** -0.5, 0.1875, ((0, 64), (1, 4)))
    out_gain = jnp.clip(1.0 + 0.18 * jax.random.normal(key_list[12], (D,), jnp.float32), 0.1, 1.9)
    return {"queries": queries, "keys": keys, "values": values, "break_bias": break_bias, "residual": residual, "w_out": w_out, "ffn_gain": ffn_gain, "pick_ids": pick_ids, "pair_logit": pair_logit, "w_gate": w_gate, "w_up": w_up, "w_down": w_down, "out_gain": out_gain}


epsilon = 1e-06

def rounded(values_in):
    return lax.optimization_barrier(values_in.astype(jnp.bfloat16)).astype(jnp.float32)

def stick_block(carried, query_rows, key_block, value_block, head_bias, query_pos, key_pos):
    output, used_up = carried
    scores = jnp.einsum('qcgd,scd->qcgs', query_rows.astype(jnp.float32), key_block.astype(jnp.float32))
    scores = scores * query_rows.shape[-1] ** (-0.5) + head_bias[None, :, :, None]
    before = (key_pos[None, :] < query_pos[:, None])[:, None, None, :]
    breaks = jnp.where(before, jax.nn.softplus(scores), 0.0)
    behind = lax.cumsum(breaks, axis=3, reverse=True) - breaks
    weights = jnp.where(before, jnp.exp(jax.nn.log_sigmoid(scores) - behind - used_up[..., None]), 0.0)
    output = output + jnp.einsum('qcgs,scd->qcgd', rounded(weights), value_block.astype(jnp.float32))
    return (output, used_up + lax.optimization_barrier(jnp.sum(breaks, axis=3)))

def reference(queries, keys, values, break_bias, residual, w_out, ffn_gain, pick_ids, pair_logit, w_gate, w_up, w_down, out_gain):
    extent = queries.shape[0]
    per_key = HEADS // KV_HEADS
    window = min(512, extent)
    blocks = extent // window
    query_all = queries.reshape(blocks, window, KV_HEADS, per_key, HEAD)
    key_all = keys.reshape(extent, KV_HEADS, HEAD)
    value_all = values.reshape(extent, KV_HEADS, HEAD)
    head_bias = break_bias.reshape(KV_HEADS, per_key)

    def one_block(block_index):
        query_rows = lax.dynamic_index_in_dim(query_all, block_index, 0, keepdims=False)
        query_pos = block_index * window + jnp.arange(window, dtype=jnp.int32)
        initial = (jnp.zeros((window, KV_HEADS, per_key, HEAD), jnp.float32), jnp.zeros((window, KV_HEADS, per_key), jnp.float32))

        def visit(step_index, carried):
            first_key = ((block_index - step_index) * window).astype(jnp.int32)
            key_block = lax.dynamic_slice_in_dim(key_all, first_key, window, 0)
            value_block = lax.dynamic_slice_in_dim(value_all, first_key, window, 0)
            key_pos = first_key + jnp.arange(window, dtype=jnp.int32)
            return stick_block(carried, query_rows, key_block, value_block, head_bias, query_pos, key_pos)
        return lax.fori_loop(jnp.int32(0), block_index + 1, visit, initial)[0]
    attended = lax.map(one_block, jnp.arange(blocks, dtype=jnp.int32)).reshape(extent, HEADS, HEAD)
    scaled = attended * lax.rsqrt(lax.optimization_barrier(jnp.mean(attended * attended, axis=-1, keepdims=True)) + epsilon)
    head_out = scaled.astype(jnp.bfloat16).reshape(extent, HEADS * HEAD)
    set_width = HEADS * HEAD // N_TP
    mixed = jnp.zeros((extent, D), jnp.float32)
    for member in range(N_TP):
        col_start = member * set_width
        mixed = mixed + rounded(jnp.dot(head_out[:, col_start:col_start + set_width], w_out[col_start:col_start + set_width], preferred_element_type=jnp.float32))
    stream = (residual.astype(jnp.float32) + mixed).astype(jnp.bfloat16)
    stream_float = stream.astype(jnp.float32)
    ffn_in = (stream_float * lax.rsqrt(lax.optimization_barrier(jnp.mean(stream_float * stream_float, axis=-1, keepdims=True)) + epsilon) * ffn_gain).astype(jnp.bfloat16)
    picks_flat = pick_ids.reshape(-1).astype(jnp.int32)
    total_picks = picks_flat.shape[0]
    ordering = jnp.argsort(picks_flat, stable=True).astype(jnp.int32)
    sorted_ids = picks_flat[ordering]
    tallies = lax.optimization_barrier(jnp.sum((picks_flat[None, :] == jnp.arange(EXPERTS, dtype=jnp.int32)[:, None]).astype(jnp.int32), axis=1)).astype(jnp.int32)
    offsets = (jnp.cumsum(tallies) - tallies).astype(jnp.int32)
    within = (jnp.arange(total_picks, dtype=jnp.int32) - offsets[sorted_ids]).astype(jnp.int32)
    room = N_SP * N_TP * CAP
    table = jnp.full((EXPERTS, room), total_picks, jnp.int32).at[sorted_ids, within].set(ordering)
    padded = jnp.concatenate([ffn_in, jnp.zeros((1, D), jnp.bfloat16)], axis=0)
    unit_width = FF // N_TP

    def run_expert(operands):
        row_ids, gate_matrix, up_matrix, down_matrix = operands
        inputs = padded[row_ids // TOP]
        hidden = (jax.nn.silu(jnp.dot(inputs, gate_matrix, preferred_element_type=jnp.float32)) * jnp.dot(inputs, up_matrix, preferred_element_type=jnp.float32)).astype(jnp.bfloat16)
        summed = jnp.zeros((room, D), jnp.float32)
        for member in range(N_TP):
            unit_start = member * unit_width
            summed = summed + rounded(jnp.dot(hidden[:, unit_start:unit_start + unit_width], down_matrix[unit_start:unit_start + unit_width], preferred_element_type=jnp.float32))
        return summed.astype(jnp.bfloat16)
    results = lax.map(run_expert, (table, w_gate, w_up, w_down))
    per_pick = jnp.zeros((total_picks + 1, D), jnp.bfloat16).at[table.reshape(-1)].set(results.reshape(-1, D))
    per_pick = per_pick[:total_picks].astype(jnp.float32).reshape(extent, TOP, D)
    blended = jax.nn.sigmoid(pair_logit)[:, None] * per_pick[:, 0] + jax.nn.sigmoid(-pair_logit)[:, None] * per_pick[:, 1]
    blend_scale = lax.rsqrt(lax.optimization_barrier(jnp.mean(blended * blended, axis=-1, keepdims=True)) + epsilon)
    return (stream_float + blended * blend_scale * out_gain).astype(jnp.bfloat16)
```

```python
import functools
import math

import jax
import jax.numpy as jnp
from jax import lax
from jax.experimental import pallas as pl
from jax.experimental.pallas import tpu as pltpu
from jax.sharding import PartitionSpec as P

HEAD = 128
TOP = 2


epsilon = 1e-06


def split_up(shard, dim, peers):
    before, after = (shard.shape[:dim], shard.shape[dim + 1 :])
    return jnp.moveaxis(shard.reshape(*before, peers, -1, *after), dim, 0)


def summed_on_arrival(shard, axis, dim):
    parts = split_up(shard, dim, lax.axis_size(axis))
    arrived = lax.all_to_all(parts, axis, split_axis=0, concat_axis=0, tiled=True)
    return arrived.astype(jnp.float32).sum(axis=0)


LOG2E = 1.4426950408889634
KB = 256

def attend_block(qs, k_ref, v_ref, tri, bias_ref, acc, used, pair, masked, shift):
    k = jnp.concatenate([k_ref[0, pair], k_ref[1, pair]], axis=0)
    v = jnp.concatenate([v_ref[0, pair], v_ref[1, pair]], axis=0)
    s = lax.dot_general(qs[...], k, (((1,), (1,)), ((), ())), preferred_element_type=jnp.float32)
    rows = s.shape[0] // 4
    c = LOG2E * 128 ** -0.5
    zs, hl = [], []
    if masked:
        col = lax.broadcasted_iota(jnp.int32, (rows, KB), 1)
        row = lax.broadcasted_iota(jnp.int32, (rows, KB), 0)
        before = col < row + shift
    for h in range(4):
        z = s[h * rows:(h + 1) * rows] * c + bias_ref[0, h] * LOG2E
        b = jnp.maximum(z, 0.0) + jnp.log2(1.0 + jnp.exp2(-jnp.abs(z)))
        if masked:
            b = jnp.where(before, b, 0.0)
        hi = b.astype(jnp.bfloat16)
        lo = (b - hi.astype(jnp.float32)).astype(jnp.bfloat16)
        zs.append(z)
        hl.append(jnp.concatenate([hi, lo], axis=1))
    incl = jnp.dot(jnp.concatenate(hl, axis=0), tri[...], preferred_element_type=jnp.float32)
    ws = []
    for h in range(4):
        sl = slice(h * rows, (h + 1) * rows)
        u = used[sl]
        w = jnp.exp2(zs[h] - incl[sl] - jnp.concatenate([u, u], axis=1))
        if masked:
            w = jnp.where(before, w, 0.0)
        ws.append(w.astype(jnp.bfloat16))
        used[sl] = u + jnp.broadcast_to(incl[sl, 0:1], (rows, 128))
    acc[...] += jnp.dot(jnp.concatenate(ws, axis=0), v, preferred_element_type=jnp.float32)

def attn_kernel(p_ref, bias_ref, q_ref, k_ref, v_ref, o_ref, qs, tri, acc, used):
    rows = q_ref.shape[0]
    p = p_ref[0]
    for h in range(4):
        qs[h * rows:(h + 1) * rows] = q_ref[:, h * 128:(h + 1) * 128]
    r = lax.broadcasted_iota(jnp.int32, (KB, KB), 0)
    cc = lax.broadcasted_iota(jnp.int32, (KB, KB), 1)
    t = jnp.where(r >= cc, 1.0, 0.0).astype(jnp.bfloat16)
    tri[0:KB] = t
    tri[KB:2 * KB] = t
    acc[...] = jnp.zeros_like(acc)
    used[...] = jnp.zeros_like(used)
    top = (p * rows) // KB
    attend_block(qs, k_ref, v_ref, tri, bias_ref, acc, used, top, True, p * rows - top * KB)

    def body(i, _):
        attend_block(qs, k_ref, v_ref, tri, bias_ref, acc, used, top - 1 - i, False, 0)
        return 0
    lax.fori_loop(0, top, body, 0)
    for h in range(4):
        a = acc[h * rows:(h + 1) * rows]
        sc = a * lax.rsqrt(jnp.mean(a * a, axis=-1, keepdims=True) + 1e-6)
        o_ref[:, h * 128:(h + 1) * 128] = sc.astype(jnp.bfloat16)

def attn(p, bias, q, k, v):
    rows = q.shape[0]
    return pl.pallas_call(
        attn_kernel,
        out_shape=jax.ShapeDtypeStruct((rows, 512), jnp.bfloat16),
        in_specs=[pl.BlockSpec(memory_space=pltpu.SMEM), pl.BlockSpec(memory_space=pltpu.SMEM),
                  pl.BlockSpec(memory_space=pltpu.VMEM), pl.BlockSpec(memory_space=pltpu.VMEM), pl.BlockSpec(memory_space=pltpu.VMEM)],
        out_specs=pl.BlockSpec(memory_space=pltpu.VMEM),
        scratch_shapes=[pltpu.VMEM((4 * rows, 128), jnp.bfloat16), pltpu.VMEM((2 * KB, KB), jnp.bfloat16),
                        pltpu.VMEM((4 * rows, 128), jnp.float32), pltpu.VMEM((4 * rows, 128), jnp.float32)],
        compiler_params=pltpu.CompilerParams(vmem_limit_bytes=60000 * 1024),
    )(p, bias, q, k, v)


MESH = pl.DeviceIdType.MESH
NZ, NX = 8, 4

def place():
    sp = lax.axis_index("sp")
    return sp // 8, (sp // 2) % 4, sp % 2

def device(z, x, c):
    return {"sp": z * 8 + x * 2 + c, "tp": lax.axis_index("tp")}

def gather_plan():
    zs = [("A", d) for d in (1, 2, 3, 4)] + [("B", d) for d in (1, 2, 3)]
    xs = [("A", 1), ("A", 2), ("B", 1)]
    none = ("O", 0)
    events = []
    for r in zs:
        events.append((r[1], "k", r, none, "z"))
    for rz in [none] + zs:
        for rx in xs:
            events.append((rz[1] + rx[1] + 0.25, "k", rz, rx, "x"))
    for r in xs:
        events.append((r[1], "v", none, r, "x"))
    for rx in [none] + xs:
        for rz in zs:
            events.append((rz[1] + rx[1] + 0.25, "v", rz, rx, "z"))
    return sorted(events)

def gather_kernel(k_ref, v_ref, kall, vall, ssem, rsem):
    z, x, c = place()
    sgn = 1 - 2 * c
    step = {"A": sgn, "B": -sgn, "O": 0}
    barrier = pltpu.get_barrier_semaphore()
    zn = {"A": (z + sgn + NZ) % NZ, "B": (z - sgn + NZ) % NZ}
    xn = {"A": (x + sgn + NX) % NX, "B": (x - sgn + NX) % NX}
    peers = [device(zn["A"], x, c), device(zn["B"], x, c), device(z, xn["A"], c), device(z, xn["B"], c), device(z, x, 1 - c)]
    for peer in peers:
        pl.semaphore_signal(barrier, inc=1, device_id=peer, device_id_type=MESH)
    pl.semaphore_wait(barrier, 5)
    zto = {"A": peers[0], "B": peers[1]}
    xto = {"A": peers[2], "B": peers[3]}
    full = {"k": kall, "v": vall}
    own = {"k": k_ref, "v": v_ref}
    tags = {}

    def tag(key):
        return tags.setdefault(key, len(tags))

    def source(rz, rx):
        return ((z - step[rz[0]] * rz[1] + NZ) % NZ) * NX + (x - step[rx[0]] * rx[1] + NX) % NX

    sends = []

    def send(arr, rz, rx, kind, to):
        i = source(rz, rx)
        src = own[arr] if (rz[1] == 0 and rx[1] == 0) else full[arr].at[c, i]
        if kind == "z":
            key = (arr, (to, rz[1] + 1), rx, "z"); dst = zto[to]
        elif kind == "x":
            key = (arr, rz, (to, rx[1] + 1), "x"); dst = xto[to]
        else:
            key = (arr, rz, rx, "d"); dst = peers[4]
        t = tag(key)
        copy = pltpu.make_async_remote_copy(src_ref=src, dst_ref=full[arr].at[c, i], send_sem=ssem.at[t], recv_sem=rsem.at[t], device_id=dst, device_id_type=MESH)
        copy.start()
        sends.append(copy)

    def arrived(arr, rz, rx, kind):
        t = tag((arr, rz, rx, kind))
        if kind == "d":
            i = ((z + step[rz[0]] * rz[1] + NZ) % NZ) * NX + (x + step[rx[0]] * rx[1] + NX) % NX
            ref = full[arr].at[1 - c, i]
        else:
            ref = full[arr].at[c, source(rz, rx)]
        pltpu.make_async_remote_copy(src_ref=ref, dst_ref=ref, send_sem=ssem.at[t], recv_sem=rsem.at[t], device_id=peers[4], device_id_type=MESH).wait_recv()

    most = {"A": 4, "B": 3}
    mostx = {"A": 2, "B": 1}
    o = ("O", 0)
    send("k", o, o, "z", "A"); send("k", o, o, "z", "B"); send("v", o, o, "x", "A"); send("v", o, o, "x", "B")
    send("k", o, o, "x", "A"); send("k", o, o, "x", "B"); send("v", o, o, "z", "A"); send("v", o, o, "z", "B")
    send("k", o, o, "d", None); send("v", o, o, "d", None)
    me = z * NX + x
    kall[c, me] = k_ref[...]
    vall[c, me] = v_ref[...]
    dlist = [("k", o, o), ("v", o, o)]
    for _, arr, rz, rx, kind in gather_plan():
        arrived(arr, rz, rx, kind)
        if kind == "z" and rz[1] < most[rz[0]]:
            send(arr, rz, rx, "z", rz[0])
        if kind == "x" and rx[1] < mostx[rx[0]]:
            send(arr, rz, rx, "x", rx[0])
        if arr == "k" and kind == "z":
            send(arr, rz, rx, "x", "A"); send(arr, rz, rx, "x", "B")
        if arr == "v" and kind == "x":
            send(arr, rz, rx, "z", "A"); send(arr, rz, rx, "z", "B")
        send(arr, rz, rx, "d", None)
        dlist.append((arr, rz, rx))
    for arr, rz, rx in dlist:
        arrived(arr, rz, rx, "d")
    for s in sends:
        s.wait_send()

def gather(k, v):
    rows, width = k.shape
    out = jax.ShapeDtypeStruct((2, NZ * NX, rows, width), k.dtype)
    vm = pl.BlockSpec(memory_space=pltpu.VMEM)
    return pl.pallas_call(
        gather_kernel, out_shape=(out, out), in_specs=[vm, vm], out_specs=(vm, vm),
        scratch_shapes=[pltpu.SemaphoreType.DMA((128,)), pltpu.SemaphoreType.DMA((128,))],
        compiler_params=pltpu.CompilerParams(collective_id=0, has_side_effects=True, vmem_limit_bytes=32 * 1024 * 1024),
    )(k, v)


def on_device(
    queries,
    keys,
    values,
    break_bias,
    residual,
    w_out,
    ffn_gain,
    pick_ids,
    pair_logit,
    w_gate,
    w_up,
    w_down,
    out_gain,
):
    length = queries.shape[0]
    position = lax.axis_index("sp").astype(jnp.int32).reshape(1)
    key_all, value_all = gather(keys, values)
    head_out = attn(position, break_bias.reshape(1, 4), queries, key_all, value_all)
    quarters = lax.axis_size("tp")
    quarter = lax.axis_index("tp")
    slice_rows = length // quarters
    width = w_out.shape[1]
    experts = lax.axis_size("sp")
    capacity = max(2, (3 * slice_rows + experts - 1) // experts)
    mixed = summed_on_arrival(
        jnp.dot(head_out, w_out, preferred_element_type=jnp.float32).astype(jnp.bfloat16), "tp", 0
    )
    stream = (residual.astype(jnp.float32) + mixed).astype(jnp.bfloat16)
    routed = lax.dynamic_slice_in_dim(pick_ids, quarter * slice_rows, slice_rows, 0)[None]
    stream_float = stream.astype(jnp.float32)
    ffn_in = (
        stream_float
        * lax.rsqrt(jnp.mean(stream_float * stream_float, axis=-1, keepdims=True) + epsilon)
        * ffn_gain
    ).astype(jnp.bfloat16)
    blocks = routed.shape[0]
    entries = ffn_in.reshape(blocks, slice_rows, width)
    flat_ids = routed.reshape(blocks, slice_rows * TOP)
    places = jnp.arange(slice_rows * TOP, dtype=jnp.int32)
    earlier = places[None, :] < places[:, None]
    matches = (flat_ids[:, :, None] == flat_ids[:, None, :]) & earlier[None]
    ranks = jnp.sum(matches.astype(jnp.int32), axis=2)
    targets = (flat_ids * capacity + ranks).reshape(blocks, slice_rows, TOP)
    block_ids = jnp.arange(blocks, dtype=jnp.int32)[:, None]
    outgoing = jnp.zeros((blocks, experts * capacity, width), jnp.bfloat16)
    for pick_index in range(TOP):
        outgoing = outgoing.at[block_ids, targets[:, :, pick_index]].set(entries)
    arrived = lax.all_to_all(outgoing, "sp", split_axis=1, concat_axis=1, tiled=True).reshape(
        -1, width
    )
    piece = lax.all_gather(arrived, "tp", axis=0, tiled=True)
    gated = jax.nn.silu(jnp.dot(piece, w_gate[0], preferred_element_type=jnp.float32))
    hidden = (gated * jnp.dot(piece, w_up[0], preferred_element_type=jnp.float32)).astype(
        jnp.bfloat16
    )
    results = summed_on_arrival(
        jnp.dot(hidden, w_down[0], preferred_element_type=jnp.float32).astype(jnp.bfloat16), "tp", 0
    ).astype(jnp.bfloat16)
    returned = lax.all_to_all(results, "sp", split_axis=0, concat_axis=0, tiled=True)
    own_targets = targets[0]
    logits = lax.dynamic_slice_in_dim(pair_logit, quarter * slice_rows, slice_rows, 0)
    leading = returned[own_targets[:, 0]].astype(jnp.float32)
    trailing = returned[own_targets[:, 1]].astype(jnp.float32)
    blended = (
        jax.nn.sigmoid(logits)[:, None] * leading + jax.nn.sigmoid(-logits)[:, None] * trailing
    )
    blend_scale = lax.rsqrt(jnp.mean(blended * blended, axis=-1, keepdims=True) + epsilon)
    return (stream_float + blended * blend_scale * out_gain).astype(jnp.bfloat16)


def solution(mesh):
    placed = (
        P("sp", "tp"),
        P("sp", "tp"),
        P("sp", "tp"),
        P("tp"),
        P(("sp", "tp"), None),
        P("tp", None),
        P(),
        P("sp", None),
        P("sp"),
        P("sp", None, "tp"),
        P("sp", None, "tp"),
        P("sp", "tp", None),
        P(),
    )
    return jax.shard_map(
        on_device, mesh=mesh, in_specs=placed, out_specs=P(("sp", "tp"), None), check_vma=False
    )
```

```python
import jax
import jax.numpy as jnp
from jax import lax
from jax.experimental import pallas as pl
from jax.experimental.pallas import tpu as pltpu
from jax.sharding import PartitionSpec as P

LOG2E = 1.4426950408889634
KB = 256

def attend_block(qs, k_ref, v_ref, tri, bias_ref, acc, used, pair, masked, shift):
    k = jnp.concatenate([k_ref[0, pair], k_ref[1, pair]], axis=0)
    v = jnp.concatenate([v_ref[0, pair], v_ref[1, pair]], axis=0)
    s = lax.dot_general(qs[...], k, (((1,), (1,)), ((), ())), preferred_element_type=jnp.float32)
    rows = s.shape[0] // 4
    c = LOG2E * 128 ** -0.5
    zs, hl = [], []
    if masked:
        col = lax.broadcasted_iota(jnp.int32, (rows, KB), 1)
        row = lax.broadcasted_iota(jnp.int32, (rows, KB), 0)
        before = col < row + shift
    for h in range(4):
        z = s[h * rows:(h + 1) * rows] * c + bias_ref[0, h] * LOG2E
        b = jnp.maximum(z, 0.0) + jnp.log2(1.0 + jnp.exp2(-jnp.abs(z)))
        if masked:
            b = jnp.where(before, b, 0.0)
        hi = b.astype(jnp.bfloat16)
        lo = (b - hi.astype(jnp.float32)).astype(jnp.bfloat16)
        zs.append(z)
        hl.append(jnp.concatenate([hi, lo], axis=1))
    incl = jnp.dot(jnp.concatenate(hl, axis=0), tri[...], preferred_element_type=jnp.float32)
    ws = []
    for h in range(4):
        sl = slice(h * rows, (h + 1) * rows)
        u = used[sl]
        w = jnp.exp2(zs[h] - incl[sl] - jnp.concatenate([u, u], axis=1))
        if masked:
            w = jnp.where(before, w, 0.0)
        ws.append(w.astype(jnp.bfloat16))
        used[sl] = u + jnp.broadcast_to(incl[sl, 0:1], (rows, 128))
    acc[...] += jnp.dot(jnp.concatenate(ws, axis=0), v, preferred_element_type=jnp.float32)

def attn_kernel(p_ref, bias_ref, q_ref, k_ref, v_ref, o_ref, qs, tri, acc, used):
    rows = q_ref.shape[0]
    p = p_ref[0]
    for h in range(4):
        qs[h * rows:(h + 1) * rows] = q_ref[:, h * 128:(h + 1) * 128]
    r = lax.broadcasted_iota(jnp.int32, (KB, KB), 0)
    cc = lax.broadcasted_iota(jnp.int32, (KB, KB), 1)
    t = jnp.where(r >= cc, 1.0, 0.0).astype(jnp.bfloat16)
    tri[0:KB] = t
    tri[KB:2 * KB] = t
    acc[...] = jnp.zeros_like(acc)
    used[...] = jnp.zeros_like(used)
    top = (p * rows) // KB
    attend_block(qs, k_ref, v_ref, tri, bias_ref, acc, used, top, True, p * rows - top * KB)

    def body(i, _):
        attend_block(qs, k_ref, v_ref, tri, bias_ref, acc, used, top - 1 - i, False, 0)
        return 0
    lax.fori_loop(0, top, body, 0)
    for h in range(4):
        a = acc[h * rows:(h + 1) * rows]
        sc = a * lax.rsqrt(jnp.mean(a * a, axis=-1, keepdims=True) + 1e-6)
        o_ref[:, h * 128:(h + 1) * 128] = sc.astype(jnp.bfloat16)

def attn(p, bias, q, k, v):
    rows = q.shape[0]
    return pl.pallas_call(
        attn_kernel,
        out_shape=jax.ShapeDtypeStruct((rows, 512), jnp.bfloat16),
        in_specs=[pl.BlockSpec(memory_space=pltpu.SMEM), pl.BlockSpec(memory_space=pltpu.SMEM),
                  pl.BlockSpec(memory_space=pltpu.VMEM), pl.BlockSpec(memory_space=pltpu.VMEM), pl.BlockSpec(memory_space=pltpu.VMEM)],
        out_specs=pl.BlockSpec(memory_space=pltpu.VMEM),
        scratch_shapes=[pltpu.VMEM((4 * rows, 128), jnp.bfloat16), pltpu.VMEM((2 * KB, KB), jnp.bfloat16),
                        pltpu.VMEM((4 * rows, 128), jnp.float32), pltpu.VMEM((4 * rows, 128), jnp.float32)],
        compiler_params=pltpu.CompilerParams(vmem_limit_bytes=60000 * 1024),
    )(p, bias, q, k, v)


MESH = pl.DeviceIdType.MESH
NZ, NX = 8, 4

def place():
    sp = lax.axis_index("sp")
    return sp // 8, (sp // 2) % 4, sp % 2

def device(z, x, c):
    return {"sp": z * 8 + x * 2 + c, "tp": lax.axis_index("tp")}

def gather_plan():
    zs = [("A", d) for d in (1, 2, 3, 4)] + [("B", d) for d in (1, 2, 3)]
    xs = [("A", 1), ("A", 2), ("B", 1)]
    none = ("O", 0)
    events = []
    for r in zs:
        events.append((r[1], "k", r, none, "z"))
    for rz in [none] + zs:
        for rx in xs:
            events.append((rz[1] + rx[1] + 0.25, "k", rz, rx, "x"))
    for r in xs:
        events.append((r[1], "v", none, r, "x"))
    for rx in [none] + xs:
        for rz in zs:
            events.append((rz[1] + rx[1] + 0.25, "v", rz, rx, "z"))
    return sorted(events)

def gather_kernel(k_ref, v_ref, down_ref, kall, vall, down, relay, ssem, rsem, dsend, drecv, lsem):
    z, x, c = place()
    sgn = 1 - 2 * c
    step = {"A": sgn, "B": -sgn, "O": 0}
    barrier = pltpu.get_barrier_semaphore()
    zn = {"A": (z + sgn + NZ) % NZ, "B": (z - sgn + NZ) % NZ}
    xn = {"A": (x + sgn + NX) % NX, "B": (x - sgn + NX) % NX}
    y, right, left, over = y_ring()
    to_y = [{"sp": lax.axis_index("sp"), "tp": t} for t in (right, left)]
    peers = [device(zn["A"], x, c), device(zn["B"], x, c), device(z, xn["A"], c), device(z, xn["B"], c), device(z, x, 1 - c)]
    for peer in peers + to_y:
        pl.semaphore_signal(barrier, inc=1, device_id=peer, device_id_type=MESH)
    pl.semaphore_wait(barrier, 7)

    def columns(t):
        return pl.ds(pl.multiple_of(t * 1024, 1024), 1024)

    def across(n, src, dst, to):
        return pltpu.make_async_remote_copy(src_ref=src, dst_ref=dst, send_sem=dsend.at[n], recv_sem=drecv.at[n], device_id=to_y[to], device_id_type=MESH)

    down_copies = [
        across(0, down_ref.at[0:128, columns(over)], relay.at[0], 0),
        across(1, down_ref.at[128:256, columns(over)], relay.at[1], 1),
        across(2, down_ref.at[:, columns(right)], down.at[y], 0),
        across(3, down_ref.at[:, columns(left)], down.at[y], 1),
    ]
    passed_on = [across(4, relay.at[0], down.at[left, 0:128], 0), across(5, relay.at[1], down.at[right, 128:256], 1)]
    arrivals = [
        across(2, down.at[left], down.at[left], 0), across(3, down.at[right], down.at[right], 1),
        across(4, down.at[over, 0:128], down.at[over, 0:128], 0), across(5, down.at[over, 128:256], down.at[over, 128:256], 1),
    ]
    own_down = pltpu.make_async_copy(down_ref.at[:, columns(y)], down.at[y], lsem)
    zto = {"A": peers[0], "B": peers[1]}
    xto = {"A": peers[2], "B": peers[3]}
    full = {"k": kall, "v": vall}
    own = {"k": k_ref, "v": v_ref}
    tags = {}

    def tag(key):
        return tags.setdefault(key, len(tags))

    def source(rz, rx):
        return ((z - step[rz[0]] * rz[1] + NZ) % NZ) * NX + (x - step[rx[0]] * rx[1] + NX) % NX

    sends = []

    def send(arr, rz, rx, kind, to):
        i = source(rz, rx)
        src = own[arr] if (rz[1] == 0 and rx[1] == 0) else full[arr].at[c, i]
        if kind == "z":
            key = (arr, (to, rz[1] + 1), rx, "z"); dst = zto[to]
        elif kind == "x":
            key = (arr, rz, (to, rx[1] + 1), "x"); dst = xto[to]
        else:
            key = (arr, rz, rx, "d"); dst = peers[4]
        t = tag(key)
        copy = pltpu.make_async_remote_copy(src_ref=src, dst_ref=full[arr].at[c, i], send_sem=ssem.at[t], recv_sem=rsem.at[t], device_id=dst, device_id_type=MESH)
        copy.start()
        sends.append(copy)

    def arrived(arr, rz, rx, kind):
        t = tag((arr, rz, rx, kind))
        if kind == "d":
            i = ((z + step[rz[0]] * rz[1] + NZ) % NZ) * NX + (x + step[rx[0]] * rx[1] + NX) % NX
            ref = full[arr].at[1 - c, i]
        else:
            ref = full[arr].at[c, source(rz, rx)]
        pltpu.make_async_remote_copy(src_ref=ref, dst_ref=ref, send_sem=ssem.at[t], recv_sem=rsem.at[t], device_id=peers[4], device_id_type=MESH).wait_recv()

    most = {"A": 4, "B": 3}
    mostx = {"A": 2, "B": 1}
    o = ("O", 0)
    send("k", o, o, "z", "A"); send("k", o, o, "z", "B"); send("v", o, o, "x", "A"); send("v", o, o, "x", "B")
    send("k", o, o, "x", "A"); send("k", o, o, "x", "B"); send("v", o, o, "z", "A"); send("v", o, o, "z", "B")
    send("k", o, o, "d", None); send("v", o, o, "d", None)
    for it in down_copies:
        it.start()
    own_down.start()
    me = z * NX + x
    kall[c, me] = k_ref[...]
    vall[c, me] = v_ref[...]
    dlist = [("k", o, o), ("v", o, o)]
    for n, (_, arr, rz, rx, kind) in enumerate(gather_plan()):
        if n == 24:
            for way in (0, 1):
                down_copies[way].wait_recv()
                passed_on[way].start()
        arrived(arr, rz, rx, kind)
        if kind == "z" and rz[1] < most[rz[0]]:
            send(arr, rz, rx, "z", rz[0])
        if kind == "x" and rx[1] < mostx[rx[0]]:
            send(arr, rz, rx, "x", rx[0])
        if arr == "k" and kind == "z":
            send(arr, rz, rx, "x", "A"); send(arr, rz, rx, "x", "B")
        if arr == "v" and kind == "x":
            send(arr, rz, rx, "z", "A"); send(arr, rz, rx, "z", "B")
        send(arr, rz, rx, "d", None)
        dlist.append((arr, rz, rx))
    for arr, rz, rx in dlist:
        arrived(arr, rz, rx, "d")
    for it in arrivals:
        it.wait_recv()
    own_down.wait()
    for it in sends + down_copies + passed_on:
        it.wait_send()

def gather(k, v, down):
    rows, width = k.shape
    out = jax.ShapeDtypeStruct((2, NZ * NX, rows, width), k.dtype)
    vm = pl.BlockSpec(memory_space=pltpu.VMEM)
    dma = pltpu.SemaphoreType.DMA
    return pl.pallas_call(
        gather_kernel, out_shape=(out, out, jax.ShapeDtypeStruct((4, 256, 1024), k.dtype)),
        in_specs=[vm, vm, pl.BlockSpec(memory_space=pl.ANY)], out_specs=(vm, vm, vm),
        scratch_shapes=[pltpu.VMEM((2, 128, 1024), k.dtype), dma((128,)), dma((128,)), dma((6,)), dma((6,)), dma],
        compiler_params=pltpu.CompilerParams(collective_id=0, has_side_effects=True, vmem_limit_bytes=32 * 1024 * 1024),
    )(k, v, down)


def y_ring():
    y = lax.axis_index("tp")
    return y, (y + 1) % 4, (y + 3) % 4, (y + 2) % 4


def slot_columns(pick_ref):
    rows = lax.broadcasted_iota(jnp.int32, (128, 128), 0)
    lanes = lax.broadcasted_iota(jnp.int32, (128, 128), 1)
    earlier = (lanes < rows) & ((lanes & 96) == (rows & 96))
    wide = [jnp.broadcast_to(pick_ref[:, k : k + 1], (128, 128)) for k in range(2)]
    across = [w.astype(jnp.float32).T.astype(jnp.int32) for w in wide]
    hits = []
    for w in wide:
        same = earlier & ((across[0] == w) | (across[1] == w))
        rank = jnp.sum(jnp.where(same, 1.0, 0.0), axis=1, keepdims=True).astype(jnp.int32)
        slot = (w & 7) * 16 + (w >> 3) * 2 + rank
        hits.append(slot == lanes)
    return hits


def mix_kernel(head_ref, w_ref, res_ref, gain_ref, pick_ref, stream_ref, disp_ref,
               part, from_left, from_right, relay, summed, slots, ssem, rsem):
    y, right, left, over = y_ring()
    sp = lax.axis_index("sp")
    barrier = pltpu.get_barrier_semaphore()
    for t in (right, left):
        pl.semaphore_signal(barrier, inc=1, device_id={"sp": sp, "tp": t}, device_id_type=MESH)
    pl.semaphore_wait(barrier, 2)

    def copy(n, src, dst, to):
        return pltpu.make_async_remote_copy(src_ref=src, dst_ref=dst, send_sem=ssem.at[n], recv_sem=rsem.at[n],
                                            device_id={"sp": sp, "tp": to}, device_id_type=MESH)

    def project(n):
        p = jnp.dot(head_ref[...], w_ref[:, n * 1024:(n + 1) * 1024], preferred_element_type=jnp.float32).astype(jnp.bfloat16)
        for t in range(4):
            part[t, n // 2, :, (n % 2) * 1024:(n % 2 + 1) * 1024] = p[32 * t:32 * t + 32]

    copies = [
        copy(0, part.at[over, 0], relay.at[0], right),
        copy(1, part.at[over, 1], relay.at[1], left),
        copy(2, part.at[right, 1], from_left.at[1], right),
        copy(3, part.at[left, 0], from_right.at[0], left),
        copy(4, summed.at[0], from_left.at[0], right),
        copy(5, summed.at[1], from_right.at[1], left),
    ]
    project(0)
    project(1)
    copies[0].start()
    copies[3].start()
    project(2)
    project(3)
    copies[1].start()
    copies[2].start()
    hits = slot_columns(pick_ref)
    slots[...] = jnp.where(hits[0] | hits[1], 1.0, 0.0).astype(jnp.bfloat16)
    copies[0].wait_recv()
    summed[0] = (part[right, 0].astype(jnp.float32) + relay[0].astype(jnp.float32)).astype(jnp.bfloat16)
    copies[4].start()
    copies[1].wait_recv()
    summed[1] = (part[left, 1].astype(jnp.float32) + relay[1].astype(jnp.float32)).astype(jnp.bfloat16)
    copies[5].start()
    for n in (2, 3, 4, 5):
        copies[n].wait_recv()
    square = jnp.zeros((32, 1), jnp.float32)
    for h in range(2):
        cols = slice(h * 2048, (h + 1) * 2048)
        mixed = part[y, h].astype(jnp.float32) + from_left[h].astype(jnp.float32) + from_right[h].astype(jnp.float32)
        s = (res_ref[:, cols].astype(jnp.float32) + mixed).astype(jnp.bfloat16)
        stream_ref[:, cols] = s
        sf = s.astype(jnp.float32)
        square = square + jnp.sum(sf * sf, axis=1, keepdims=True)
    scale = lax.rsqrt(square * (1.0 / 4096) + 1e-6)
    own = slots[pl.ds(pl.multiple_of(y * 32, 32), 32), :]
    for n in range(4):
        cols = slice(n * 1024, (n + 1) * 1024)
        f = (stream_ref[:, cols].astype(jnp.float32) * scale * gain_ref[:, cols]).astype(jnp.bfloat16)
        d = lax.dot_general(own, f, (((0,), (0,)), ((), ())), preferred_element_type=jnp.float32)
        disp_ref[:, :, cols] = d.astype(jnp.bfloat16).reshape(8, 16, 1024)
    for c in copies:
        c.wait_send()


def mix(head_out, w_out, residual, gain, picks):
    vm = pl.BlockSpec(memory_space=pltpu.VMEM)
    bf = jnp.bfloat16
    return pl.pallas_call(
        mix_kernel,
        out_shape=(jax.ShapeDtypeStruct((32, 4096), bf), jax.ShapeDtypeStruct((8, 16, 4096), bf)),
        in_specs=[vm] * 5, out_specs=(vm, vm),
        scratch_shapes=[pltpu.VMEM((4, 2, 32, 2048), bf), pltpu.VMEM((2, 32, 2048), bf), pltpu.VMEM((2, 32, 2048), bf),
                        pltpu.VMEM((2, 32, 2048), bf), pltpu.VMEM((2, 32, 2048), bf), pltpu.VMEM((128, 128), bf),
                        pltpu.SemaphoreType.DMA((6,)), pltpu.SemaphoreType.DMA((6,))],
        compiler_params=pltpu.CompilerParams(collective_id=1, has_side_effects=True, vmem_limit_bytes=40 * 1024 * 1024),
    )(head_out, w_out, residual, gain, picks)


OFFS = (0, 1, -1, 2, -2, 3, -3, 4)


def expert_kernel(disp_ref, stream_ref, gate_ref, up_ref, down_ref, gain_ref, pick_ref, logit_ref, out_ref,
                  recv_x, send_z, rows, hid, result, recv_r, send_x, recv_b, blend, send_f, fin, ssem, rsem):
    y, right, left, over = y_ring()
    z, x, c = place()
    sp = lax.axis_index("sp")
    j = x * 2 + c
    bf, f32 = jnp.bfloat16, jnp.float32
    plane = [(z, (x + o // 2) % 4, (c + o) % 2) for o in range(8)]
    column = [((z + d) % 8, x, c) for d in range(8)]
    barrier = pltpu.get_barrier_semaphore()
    for p in plane[1:] + column[1:]:
        pl.semaphore_signal(barrier, inc=1, device_id=device(*p), device_id_type=MESH)
    for t in (right, left, over):
        pl.semaphore_signal(barrier, inc=1, device_id={"sp": sp, "tp": t}, device_id_type=MESH)
    tags = {}
    sent = []

    def copy(key, src, dst, to):
        n = tags.setdefault(key, len(tags))
        return pltpu.make_async_remote_copy(src_ref=src, dst_ref=dst, send_sem=ssem.at[n], recv_sem=rsem.at[n],
                                            device_id=to, device_id_type=MESH)

    def send(key, src, dst, to):
        it = copy(key, src, dst, to)
        it.start()
        sent.append(it)

    def arrive(key, dst):
        copy(key, dst, dst, {"sp": sp, "tp": right}).wait_recv()

    to_y = {"R": {"sp": sp, "tp": right}, "L": {"sp": sp, "tp": left}, "O": {"sp": sp, "tp": over}}
    a = lax.broadcasted_iota(jnp.int32, (128, 128), 0)
    b = lax.broadcasted_iota(jnp.int32, (128, 128), 1)
    swap = jnp.where(b == ((a >> 1) & 7) * 16 + (a >> 4) * 2 + (a & 1), 1.0, 0.0).astype(bf)
    pl.semaphore_wait(barrier, 17)

    for o in (4, 5, 2, 3, 6, 7, 1):
        zz, xx, cc = plane[o]
        send(("x", o), disp_ref.at[xx * 2 + cc], recv_x.at[j], device(zz, xx, cc))
    recv_x[j] = disp_ref[j]
    hits = slot_columns(pick_ref)
    logit = jnp.broadcast_to(logit_ref[...], (128, 128)).T
    w = jnp.where(hits[0], jax.nn.sigmoid(logit), 0.0) + jnp.where(hits[1], jax.nn.sigmoid(-logit), 0.0)
    hi = w.astype(bf)
    blend[:, 0:128] = hi
    blend[:, 128:256] = (w - hi.astype(f32)).astype(bf)
    for o in (1, 2, 3, 6, 7, 4, 5):
        src = ((x - o // 2 + 4) % 4) * 2 + (c + o) % 2
        arrive(("x", o), recv_x.at[src])
    for n in range(4):
        cols = slice(n * 1024, (n + 1) * 1024)
        p = jnp.dot(swap, recv_x[:, :, cols].reshape(128, 1024), preferred_element_type=f32)
        send_z[:, :, cols] = p.astype(bf).reshape(8, 16, 1024)

    for o in range(1, 8):
        zz = (z - OFFS[o] + 8) % 8
        send(("z", o), send_z.at[zz], rows.at[o, y], device(zz, x, c))
    rows[0, y] = send_z[z]

    def gather_own(g):
        for o in (2 * g, 2 * g + 1):
            if o:
                arrive(("z", o), rows.at[o, y])
            for way in "RL":
                send(("g", way, o), rows.at[o, y], rows.at[o, y], to_y[way])

    def gather_on(g):
        for o in (2 * g, 2 * g + 1):
            arrive(("g", "R", o), rows.at[o, left])
            half = rows.at[o, left, :, 0:2048]
            send(("h", "R", o), half, half, to_y["R"])
            arrive(("g", "L", o), rows.at[o, right])
            half = rows.at[o, right, :, 2048:4096]
            send(("h", "L", o), half, half, to_y["L"])

    def hidden(g):
        for o in (2 * g, 2 * g + 1):
            arrive(("h", "R", o), rows.at[o, over, :, 0:2048])
            arrive(("h", "L", o), rows.at[o, over, :, 2048:4096])
        v = rows[2 * g:2 * g + 2].reshape(128, 4096)
        gate = jnp.dot(v, gate_ref[...], preferred_element_type=f32)
        up = jnp.dot(v, up_ref[...], preferred_element_type=f32)
        hid[g, y] = (gate / (1.0 + jnp.exp(-gate)) * up).astype(bf)
        for way in "RL":
            send(("u", way, g), hid.at[g, y], hid.at[g, y], to_y[way])

    def hidden_on(g):
        arrive(("u", "R", g), hid.at[g, left])
        half = hid.at[g, left, 0:64]
        send(("v", "R", g), half, half, to_y["R"])
        arrive(("u", "L", g), hid.at[g, right])
        half = hid.at[g, right, 64:128]
        send(("v", "L", g), half, half, to_y["L"])

    def outputs(g):
        arrive(("v", "R", g), hid.at[g, over, 0:64])
        arrive(("v", "L", g), hid.at[g, over, 64:128])
        h = jnp.concatenate([hid[g, t] for t in range(4)], axis=1)
        r = jnp.dot(h, down_ref[...].reshape(1024, 1024), preferred_element_type=f32)
        result[2 * g:2 * g + 2] = r.astype(bf).reshape(2, 4, 16, 1024)
        for o in (2 * g, 2 * g + 1):
            if o:
                zz = (z + OFFS[o] + 8) % 8
                send(("r", o), result.at[o], recv_r.at[z], device(zz, x, c))
            else:
                recv_r[z] = result[0]

    for p in range(8):
        if p < 4:
            gather_own(p)
        if 0 <= p - 1 < 4:
            gather_on(p - 1)
        if 0 <= p - 2 < 4:
            hidden(p - 2)
        if 0 <= p - 3 < 4:
            hidden_on(p - 3)
        if 0 <= p - 4 < 4:
            outputs(p - 4)

    for o in range(1, 8):
        arrive(("r", o), recv_r.at[(z - OFFS[o] + 8) % 8])
    for t in range(4):
        p = jnp.dot(swap, recv_r[:, t].reshape(128, 1024), preferred_element_type=f32)
        send_x[:, t] = p.astype(bf).reshape(8, 16, 1024)
    for o in (4, 5, 2, 3, 6, 7, 1):
        zz, xx, cc = plane[o]
        send(("b", o), send_x.at[xx * 2 + cc], recv_b.at[j], device(zz, xx, cc))
    recv_b[j] = send_x[j]
    for o in (1, 2, 3, 6, 7, 4, 5):
        src = ((x - o // 2 + 4) % 4) * 2 + (c + o) % 2
        arrive(("b", o), recv_b.at[src])

    def blended(t):
        v = recv_b[:, t].reshape(128, 1024)
        w = blend[pl.ds(pl.multiple_of(t * 32, 32), 32), :]
        return (jnp.dot(w[:, 0:128], v, preferred_element_type=f32)
                + jnp.dot(w[:, 128:256], v, preferred_element_type=f32)).astype(bf)

    for way, t in (("O", over), ("R", right), ("L", left)):
        send_f[t] = blended(t)
        send(("f", way), send_f.at[t], fin.at[y], to_y[way])
    fin[y] = blended(y)
    for way, t in (("R", left), ("L", right), ("O", over)):
        arrive(("f", way), fin.at[t])
    square = jnp.zeros((32, 1), f32)
    for t in range(4):
        v = fin[t].astype(f32)
        square = square + jnp.sum(v * v, axis=1, keepdims=True)
    scale = lax.rsqrt(square * (1.0 / 4096) + 1e-6)
    for t in range(4):
        cols = slice(t * 1024, (t + 1) * 1024)
        out_ref[:, cols] = (stream_ref[:, cols].astype(f32) + fin[t].astype(f32) * scale * gain_ref[:, cols]).astype(bf)
    for it in sent:
        it.wait_send()


def experts(disp, stream, gate, up, down, gain, picks, logits):
    vm = pl.BlockSpec(memory_space=pltpu.VMEM)
    bf = jnp.bfloat16
    sizes = [(8, 16, 4096), (8, 16, 4096), (8, 4, 16, 4096), (4, 4, 128, 256), (8, 4, 16, 1024), (8, 4, 16, 1024),
             (8, 4, 16, 1024), (8, 4, 16, 1024), (128, 256), (4, 32, 1024), (4, 32, 1024)]
    return pl.pallas_call(
        expert_kernel, out_shape=jax.ShapeDtypeStruct((32, 4096), bf), in_specs=[vm] * 8, out_specs=vm,
        scratch_shapes=[pltpu.VMEM(s, bf) for s in sizes] + [pltpu.SemaphoreType.DMA((96,)), pltpu.SemaphoreType.DMA((96,))],
        compiler_params=pltpu.CompilerParams(collective_id=2, has_side_effects=True, vmem_limit_bytes=50 * 1024 * 1024),
    )(disp, stream, gate, up, down, gain, picks, logits)


def on_device(
    queries, keys, values, break_bias, residual, w_out, ffn_gain, pick_ids, pair_logit, w_gate, w_up, w_down, out_gain
):
    position = lax.axis_index("sp").astype(jnp.int32).reshape(1)
    key_all, value_all, down = gather(keys, values, w_down[0])
    head_out = attn(position, break_bias.reshape(1, 4), queries, key_all, value_all)
    stream, disp = mix(head_out, w_out, residual, ffn_gain.reshape(1, -1), pick_ids)
    return experts(
        disp, stream, w_gate[0], w_up[0], down, out_gain.reshape(1, -1), pick_ids, pair_logit.reshape(1, -1)
    )


def solution(mesh):
    placed = (
        P("sp", "tp"),
        P("sp", "tp"),
        P("sp", "tp"),
        P("tp"),
        P(("sp", "tp"), None),
        P("tp", None),
        P(),
        P("sp", None),
        P("sp"),
        P("sp", None, "tp"),
        P("sp", None, "tp"),
        P("sp", "tp", None),
        P(),
    )
    return jax.shard_map(
        on_device, mesh=mesh, in_specs=placed, out_specs=P(("sp", "tp"), None), check_vma=False
    )
```

```python
import functools

import jax
import jax.numpy as jnp
from jax import lax
from jax.experimental import pallas as pl
from jax.experimental.pallas import tpu as pltpu
from jax.sharding import PartitionSpec as P

LOG2E = 1.4426950408889634
KB = 256

def attend_block(qs, k_ref, v_ref, tri, bias_ref, acc, used, pair, masked, shift):
    k = jnp.concatenate([k_ref[0, pair], k_ref[1, pair]], axis=0)
    v = jnp.concatenate([v_ref[0, pair], v_ref[1, pair]], axis=0)
    s = lax.dot_general(qs[...], k, (((1,), (1,)), ((), ())), preferred_element_type=jnp.float32)
    rows = s.shape[0] // 4
    c = LOG2E * 128 ** -0.5
    zs, hl = [], []
    if masked:
        col = lax.broadcasted_iota(jnp.int32, (rows, KB), 1)
        row = lax.broadcasted_iota(jnp.int32, (rows, KB), 0)
        before = col < row + shift
    for h in range(4):
        z = s[h * rows:(h + 1) * rows] * c + bias_ref[0, h] * LOG2E
        b = jnp.maximum(z, 0.0) + jnp.log2(1.0 + jnp.exp2(-jnp.abs(z)))
        if masked:
            b = jnp.where(before, b, 0.0)
        zs.append(z)
        hl.append(b.astype(jnp.bfloat16))
    incl = jnp.dot(jnp.concatenate(hl, axis=0), tri[...], preferred_element_type=jnp.float32)
    ws = []
    for h in range(4):
        sl = slice(h * rows, (h + 1) * rows)
        u = used[sl]
        w = jnp.exp2(zs[h] - incl[sl] - jnp.concatenate([u, u], axis=1))
        if masked:
            w = jnp.where(before, w, 0.0)
        ws.append(w.astype(jnp.bfloat16))
        used[sl] = u + jnp.broadcast_to(incl[sl, 0:1], (rows, 128))
    acc[...] += jnp.dot(jnp.concatenate(ws, axis=0), v, preferred_element_type=jnp.float32)

MESH = pl.DeviceIdType.MESH
NZ, NX = 8, 4

def place():
    sp = lax.axis_index("sp")
    return sp // 8, (sp // 2) % 4, sp % 2

def device(z, x, c):
    return {"sp": z * 8 + x * 2 + c, "tp": lax.axis_index("tp")}

def gather_plan():
    zs = [("A", d) for d in (1, 2, 3, 4)] + [("B", d) for d in (1, 2, 3)]
    xs = [("A", 1), ("A", 2), ("B", 1)]
    none = ("O", 0)
    events = []
    for r in zs:
        events.append((r[1], "k", r, none, "z"))
    for rz in [none] + zs:
        for rx in xs:
            events.append((rz[1] + rx[1] + 0.25, "k", rz, rx, "x"))
    for r in xs:
        events.append((r[1], "v", none, r, "x"))
    for rx in [none] + xs:
        for rz in zs:
            events.append((rz[1] + rx[1] + 0.25, "v", rz, rx, "z"))
    return sorted(events)


def y_ring():
    y = lax.axis_index("tp")
    return y, (y + 1) % 4, (y + 3) % 4, (y + 2) % 4


OFFS = (0, 2, -2, 4, 3, -3, 1, -1)


def slot_columns(pick_ref, z):
    rows = lax.broadcasted_iota(jnp.int32, (128, 128), 0)
    lanes = lax.broadcasted_iota(jnp.int32, (128, 128), 1)
    earlier = (lanes < rows) & ((lanes & 96) == (rows & 96))
    across = [jnp.broadcast_to(pick_ref[k : k + 1, :], (128, 128)) for k in range(2)]
    wide = [w.astype(jnp.float32).T.astype(jnp.int32) for w in across]
    lane, late = [], []
    for w in wide:
        same = earlier & ((across[0] == w) | (across[1] == w))
        rank = jnp.sum(jnp.where(same, 1.0, 0.0), axis=1, keepdims=True).astype(jnp.int32)
        away = (z - (w >> 3)) & 7
        chunk = sum(jnp.where(away == (off & 7), o, 0) for o, off in enumerate(OFFS))
        lane.append((w & 7) * 16 + (chunk & 3) * 2 + rank)
        late.append(chunk >> 2)
    return lane, late


def layer_kernel(q_hbm, k_hbm, v_hbm, bias_hbm, res_hbm, w_hbm, gain_hbm, pick_hbm, logit_hbm, gate_hbm, up_hbm, down_ref, last_hbm,
                 out_ref,
                 q_ref, k_ref, v_ref, bias_ref, res_ref, w_ref, gain_ref, pick_ref, logit_ref, gate_ref, up_ref, last_ref,
                 stream_ref, disp_ref, down, kall, vall, qs, tri, acc, used, head, drelay, part, from_left, from_right, relay, summed, slots,
                 recv_x, send_z, got, hid, result, recv_r, send_x, recv_b, blend, send_f, fin,
                 ssem, rsem, dsend, drecv, msend, mrecv, xsend, xrecv, lsem):
    z, x, c = place()
    sp = lax.axis_index("sp")
    y, right, left, over = y_ring()
    sgn = 1 - 2 * c
    step = {"A": sgn, "B": -sgn, "O": 0}
    barrier = pltpu.get_barrier_semaphore()
    zn = {"A": (z + sgn + NZ) % NZ, "B": (z - sgn + NZ) % NZ}
    xn = {"A": (x + sgn + NX) % NX, "B": (x - sgn + NX) % NX}
    to_y = [{"sp": sp, "tp": t} for t in (right, left)]
    plane = [(z, (x + o // 2) % 4, (c + o) % 2) for o in range(8)]
    column = [((z + d) % 8, x, c) for d in range(8)]
    peers = [device(zn["A"], x, c), device(zn["B"], x, c), device(z, xn["A"], c), device(z, xn["B"], c), device(z, x, 1 - c)]
    for p in plane[1:] + column[1:]:
        pl.semaphore_signal(barrier, inc=1, device_id=device(*p), device_id_type=MESH)
    for t in (right, left, over):
        pl.semaphore_signal(barrier, inc=1, device_id={"sp": sp, "tp": t}, device_id_type=MESH)
    loads = {}
    for n, (name, src, dst) in enumerate((
        ("k", k_hbm, k_ref), ("v", v_hbm, v_ref), ("q", q_hbm, q_ref), ("bias", bias_hbm, bias_ref),
        ("picks", pick_hbm, pick_ref), ("w", w_hbm, w_ref), ("res", res_hbm, res_ref), ("gain", gain_hbm, gain_ref),
        ("gate", gate_hbm, gate_ref), ("up", up_hbm, up_ref), ("last", last_hbm, last_ref), ("logit", logit_hbm, logit_ref),
    )):
        loads[name] = pltpu.make_async_copy(src, dst, lsem.at[n + 1])
        loads[name].start()

    def columns(t):
        return pl.ds(pl.multiple_of(t * 1024, 1024), 1024)

    own_down = pltpu.make_async_copy(down_ref.at[:, columns(y)], down.at[y], lsem.at[0])
    own_down.start()
    loads["k"].wait()
    loads["v"].wait()
    pl.semaphore_wait(barrier, 17)

    def across(n, src, dst, to):
        return pltpu.make_async_remote_copy(src_ref=src, dst_ref=dst, send_sem=dsend.at[n], recv_sem=drecv.at[n], device_id=to_y[to], device_id_type=MESH)

    down_copies = [
        across(0, down_ref.at[0:128, columns(over)], drelay.at[0], 0),
        across(1, down_ref.at[128:256, columns(over)], drelay.at[1], 1),
        across(2, down_ref.at[:, columns(right)], down.at[y], 0),
        across(3, down_ref.at[:, columns(left)], down.at[y], 1),
    ]
    passed_on = [across(4, drelay.at[0], down.at[left, 0:128], 0), across(5, drelay.at[1], down.at[right, 128:256], 1)]
    down_arrivals = [
        across(2, down.at[left], down.at[left], 0), across(3, down.at[right], down.at[right], 1),
        across(4, down.at[over, 0:128], down.at[over, 0:128], 0), across(5, down.at[over, 128:256], down.at[over, 128:256], 1),
    ]
    zto = {"A": peers[0], "B": peers[1]}
    xto = {"A": peers[2], "B": peers[3]}
    full = {"k": kall, "v": vall}
    own = {"k": k_ref, "v": v_ref}
    tags = {}

    def tag(key):
        return tags.setdefault(key, len(tags))

    def source(rz, rx):
        return ((z - step[rz[0]] * rz[1] + NZ) % NZ) * NX + (x - step[rx[0]] * rx[1] + NX) % NX

    sends = []

    def send(arr, rz, rx, kind, to):
        i = source(rz, rx)
        src = own[arr] if (rz[1] == 0 and rx[1] == 0) else full[arr].at[c, i]
        if kind == "z":
            key, dst = (arr, (to, rz[1] + 1), rx, "z"), zto[to]
        elif kind == "x":
            key, dst = (arr, rz, (to, rx[1] + 1), "x"), xto[to]
        else:
            key, dst = (arr, rz, rx, "d"), peers[4]
        t = tag(key)
        copy = pltpu.make_async_remote_copy(src_ref=src, dst_ref=full[arr].at[c, i], send_sem=ssem.at[t], recv_sem=rsem.at[t], device_id=dst, device_id_type=MESH)
        copy.start()
        sends.append(copy)

    def arrived(arr, rz, rx, kind):
        t = tag((arr, rz, rx, kind))
        if kind == "d":
            i = ((z + step[rz[0]] * rz[1] + NZ) % NZ) * NX + (x + step[rx[0]] * rx[1] + NX) % NX
            ref = full[arr].at[1 - c, i]
        else:
            ref = full[arr].at[c, source(rz, rx)]
        pltpu.make_async_remote_copy(src_ref=ref, dst_ref=ref, send_sem=ssem.at[t], recv_sem=rsem.at[t], device_id=peers[4], device_id_type=MESH).wait_recv()

    most = {"A": 4, "B": 3}
    mostx = {"A": 2, "B": 1}
    o = ("O", 0)
    xs = [("A", 1), ("B", 1), ("A", 2)]
    send("k", o, o, "x", "A"); send("k", o, o, "x", "B"); send("v", o, o, "x", "A"); send("v", o, o, "x", "B")
    send("k", o, o, "d", None); send("v", o, o, "d", None)
    send("k", o, o, "z", "A"); send("k", o, o, "z", "B"); send("v", o, o, "z", "A"); send("v", o, o, "z", "B")
    me = z * NX + x
    kall[c, me] = k_ref[...]
    vall[c, me] = v_ref[...]
    loads["q"].wait()
    loads["bias"].wait()
    rows = q_ref.shape[0]
    for h in range(4):
        qs[h * rows:(h + 1) * rows] = q_ref[:, h * 128:(h + 1) * 128]
    r = lax.broadcasted_iota(jnp.int32, (KB, KB), 0)
    cc = lax.broadcasted_iota(jnp.int32, (KB, KB), 1)
    t = jnp.where(r >= cc, 1.0, 0.0).astype(jnp.bfloat16)
    tri[...] = t
    acc[...] = jnp.zeros_like(acc)
    used[...] = jnp.zeros_like(used)
    for it in down_copies:
        it.start()

    def receive(arr, rz, rx, kind):
        arrived(arr, rz, rx, kind)
        if kind == "z" and rz[1] < most[rz[0]]:
            send(arr, rz, rx, "z", rz[0])
        if kind == "x" and rx[1] < mostx[rx[0]]:
            send(arr, rz, rx, "x", rx[0])
        if arr == "k" and kind == "z":
            send(arr, rz, rx, "x", "A"); send(arr, rz, rx, "x", "B")
        if arr == "v" and kind == "x":
            send(arr, rz, rx, "z", "A"); send(arr, rz, rx, "z", "B")
        send(arr, rz, rx, "d", None)

    def ways(d):
        return [o] if d == 0 else [("A", d), ("B", d)] if d < 4 else [("A", 4)]

    def settle(d):
        for arr in "kv":
            for rx in [o] + xs:
                for rz in ways(d):
                    arrived(arr, rz, rx, "d")

    def block(d, i):
        if d == 0 and i == 0:
            attend_block(qs, kall, vall, tri, bias_ref, acc, used, me, True, c * rows)
        else:
            at = me - i if d == 0 else (z - d) * NX + 3 - i

            @pl.when(x >= i if d == 0 else z >= d)
            def _():
                attend_block(qs, kall, vall, tri, bias_ref, acc, used, at, False, 0)

    waiting = []
    plan = gather_plan()
    for n, (when, arr, rz, rx, kind) in enumerate(plan):
        if n == 20:
            for way in (0, 1):
                down_copies[way].wait_recv()
                passed_on[way].start()
        receive(arr, rz, rx, kind)
        if waiting and n % 2 == 1:
            waiting.pop(0)()
        if n + 1 == len(plan) or plan[n + 1][0] > when:
            d = when - 2.25
            if d in (0, 1, 2, 3):
                waiting.append(functools.partial(settle, int(d)))
                waiting.extend(functools.partial(block, int(d), i) for i in range(4))
    for step_of in waiting:
        step_of()
    settle(4)

    def rest(i, _):
        attend_block(qs, kall, vall, tri, bias_ref, acc, used, (z - 4) * NX + 3 - i, False, 0)
        return 0

    lax.fori_loop(0, jnp.where(z >= 4, (z - 3) * NX, 0), rest, 0)
    for h in range(4):
        a = acc[h * rows:(h + 1) * rows]
        sc = a * lax.rsqrt(jnp.mean(a * a, axis=-1, keepdims=True) + 1e-6)
        head[:, h * 128:(h + 1) * 128] = sc.astype(jnp.bfloat16)
    for it in down_arrivals:
        it.wait_recv()
    own_down.wait()
    loads["w"].wait()
    loads["res"].wait()
    loads["gain"].wait()
    loads["picks"].wait()
    def copy(n, src, dst, to):
        return pltpu.make_async_remote_copy(src_ref=src, dst_ref=dst, send_sem=msend.at[n], recv_sem=mrecv.at[n],
                                            device_id={"sp": sp, "tp": to}, device_id_type=MESH)

    def project(n):
        p = jnp.dot(head[...], w_ref[:, n * 1024:(n + 1) * 1024], preferred_element_type=jnp.float32).astype(jnp.bfloat16)
        for t in range(4):
            part[t, n // 2, :, (n % 2) * 1024:(n % 2 + 1) * 1024] = p[32 * t:32 * t + 32]

    copies = [
        copy(0, part.at[over, 0], relay.at[0], right),
        copy(1, part.at[over, 1], relay.at[1], left),
        copy(2, part.at[right, 1], from_left.at[1], right),
        copy(3, part.at[left, 0], from_right.at[0], left),
        copy(4, summed.at[0], from_left.at[0], right),
        copy(5, summed.at[1], from_right.at[1], left),
    ]
    project(0)
    project(1)
    copies[0].start()
    copies[3].start()
    project(2)
    project(3)
    copies[1].start()
    copies[2].start()
    lane, late = slot_columns(pick_ref, z)
    lanes = lax.broadcasted_iota(jnp.int32, (128, 128), 1)
    for h in range(2):
        for half in range(2):
            hit = [(lane[k] + 8 * half == lanes) & (late[k] == h) for k in range(2)]
            slots[h, half] = jnp.where(hit[0] | hit[1], 1.0, 0.0).astype(jnp.bfloat16)
    copies[0].wait_recv()
    summed[0] = (part[right, 0].astype(jnp.float32) + relay[0].astype(jnp.float32)).astype(jnp.bfloat16)
    copies[4].start()
    copies[1].wait_recv()
    summed[1] = (part[left, 1].astype(jnp.float32) + relay[1].astype(jnp.float32)).astype(jnp.bfloat16)
    copies[5].start()
    for n in (2, 3, 4, 5):
        copies[n].wait_recv()
    square = jnp.zeros((32, 1), jnp.float32)
    for h in range(2):
        cols = slice(h * 2048, (h + 1) * 2048)
        mixed = part[y, h].astype(jnp.float32) + from_left[h].astype(jnp.float32) + from_right[h].astype(jnp.float32)
        s = (res_ref[:, cols].astype(jnp.float32) + mixed).astype(jnp.bfloat16)
        stream_ref[:, cols] = s
        sf = s.astype(jnp.float32)
        square = square + jnp.sum(sf * sf, axis=1, keepdims=True)
    scale = lax.rsqrt(square * (1.0 / 4096) + 1e-6)
    tags_late = {}
    sent = []
    j = x * 2 + c
    bf, f32 = jnp.bfloat16, jnp.float32

    def late_copy(key, src, dst, to):
        n = tags_late.setdefault(key, len(tags_late))
        return pltpu.make_async_remote_copy(src_ref=src, dst_ref=dst, send_sem=xsend.at[n], recv_sem=xrecv.at[n],
                                            device_id=to, device_id_type=MESH)

    def push(key, src, dst, to):
        it = late_copy(key, src, dst, to)
        it.start()
        sent.append(it)

    def arrive(key, dst):
        late_copy(key, dst, dst, {"sp": sp, "tp": right}).wait_recv()

    way_y = {"R": {"sp": sp, "tp": right}, "L": {"sp": sp, "tp": left}, "O": {"sp": sp, "tp": over}}

    def pass_on_x(o, h):
        zz, xx, cc = plane[o]
        push(("x", o, h), disp_ref.at[h, xx * 2 + cc], recv_x.at[h, j], device(zz, xx, cc))

    own_rows = pl.ds(pl.multiple_of(y * 32, 32), 32)
    f = [(stream_ref[:, n * 2048:(n + 1) * 2048].astype(jnp.float32) * scale * gain_ref[:, n * 2048:(n + 1) * 2048]).astype(jnp.bfloat16) for n in range(2)]
    f = jnp.concatenate(f, axis=0)
    for h in range(2):
        mine = jnp.concatenate([slots[h, 0, own_rows, :], slots[h, 1, own_rows, :]], axis=0)
        d = lax.dot_general(mine, f, (((0,), (0,)), ((), ())), preferred_element_type=jnp.float32)
        disp_ref[h] = d.astype(jnp.bfloat16).reshape(8, 16, 2048)
        for o in (4, 5, 2, 3, 6, 7, 1):
            pass_on_x(o, h)
    loads["logit"].wait()
    logit = jnp.broadcast_to(logit_ref[...], (128, 128)).T
    second = ((lax.broadcasted_iota(jnp.int32, (128, 128), 0) >> 5) & 1) * 8
    chance = (jax.nn.sigmoid(logit), jax.nn.sigmoid(-logit))
    for h in range(2):
        w = sum(jnp.where((lane[k] + second == lanes) & (late[k] == h), chance[k], 0.0) for k in range(2))
        hi = w.astype(bf)
        blend[:, h * 128:(h + 1) * 128] = hi
        blend[:, 256 + h * 128:256 + (h + 1) * 128] = (w - hi.astype(f32)).astype(bf)
    a = lax.broadcasted_iota(jnp.int32, (128, 128), 0)
    b = lax.broadcasted_iota(jnp.int32, (128, 128), 1)
    outward = [jnp.where(b == ((a >> 1) & 7) * 16 + half * 8 + ((a >> 4) & 3) * 2 + (a & 1), 1.0, 0.0).astype(bf)[0:64] for half in range(2)]
    homeward = jnp.where(b == ((a >> 1) & 3) * 32 + ((a >> 3) & 1) * 16 + (a >> 4) * 2 + (a & 1), 1.0, 0.0).astype(bf)
    halves = [slice(0, 2048), slice(2048, 4096)]
    plane_order = (1, 2, 3, 6, 7, 4, 5)

    def place_of(o):
        return ((x - o // 2 + 4) % 4) * 2 + (c + o) % 2

    def over_y(o):
        for half in range(2):
            part = got.at[o, y, :, halves[half]]
            for way in "RL":
                push(("g", way, o, half), part, part, way_y[way])

    def permute(h):
        recv_x[h, j] = disp_ref[h, j]
        for o in plane_order:
            arrive(("x", o, h), recv_x.at[h, place_of(o)])
        v = recv_x[h].reshape(128, 2048)
        for half in range(2):
            p = jnp.dot(outward[half], v, preferred_element_type=f32).astype(bf).reshape(4, 16, 2048)
            send_z[4 * h:4 * h + 4, :, halves[half]] = p
            if h == 0:
                got[0, y, :, halves[half]] = p[0]
        for o in range(4 * h, 4 * h + 4):
            if o:
                push(("z", o), send_z.at[o], got.at[o, y], device((z - OFFS[o] + 8) % 8, x, c))
            else:
                over_y(0)

    def gather_own(g):
        for o in (2 * g, 2 * g + 1):
            if o:
                arrive(("z", o), got.at[o, y])
                over_y(o)

    def gather_on(g):
        for o in (2 * g, 2 * g + 1):
            for h, way, t in ((0, "R", left), (1, "L", right)):
                part = got.at[o, t, :, halves[h]]
                arrive(("g", way, o, h), part)
                push(("h", way, o), part, part, way_y[way])

    def hidden(g):
        for o in (2 * g, 2 * g + 1):
            arrive(("g", "R", o, 1), got.at[o, left, :, halves[1]])
            arrive(("g", "L", o, 0), got.at[o, right, :, halves[0]])
            arrive(("h", "R", o), got.at[o, over, :, halves[0]])
            arrive(("h", "L", o), got.at[o, over, :, halves[1]])
        v = got[2 * g:2 * g + 2].reshape(128, 4096)
        gate = jnp.dot(v, gate_ref[...], preferred_element_type=f32)
        up = jnp.dot(v, up_ref[...], preferred_element_type=f32)
        hid[g, y] = (gate / (1.0 + jnp.exp(-gate)) * up).astype(bf)
        for way in "RL":
            push(("u", way, g), hid.at[g, y], hid.at[g, y], way_y[way])

    def hidden_on(g):
        arrive(("u", "R", g), hid.at[g, left])
        half = hid.at[g, left, 0:64]
        push(("v", "R", g), half, half, way_y["R"])
        arrive(("u", "L", g), hid.at[g, right])
        half = hid.at[g, right, 64:128]
        push(("v", "L", g), half, half, way_y["L"])

    def outputs(g):
        arrive(("v", "R", g), hid.at[g, over, 0:64])
        arrive(("v", "L", g), hid.at[g, over, 64:128])
        h = jnp.concatenate([hid[g, t] for t in range(4)], axis=1)
        r = jnp.dot(h, down[...].reshape(1024, 1024), preferred_element_type=f32)
        result[2 * g:2 * g + 2] = r.astype(bf).reshape(2, 4, 16, 1024)
        for o in (2 * g, 2 * g + 1):
            if o:
                push(("r", o), result.at[o], recv_r.at[o], device((z + OFFS[o] + 8) % 8, x, c))
            else:
                recv_r[0] = result[0]

    def homeward_x(h):
        for o in range(4 * h, 4 * h + 4):
            if o:
                arrive(("r", o), recv_r.at[o])
        for t in range(2):
            v = recv_r[4 * h:4 * h + 4, 2 * t:2 * t + 2].reshape(128, 1024)
            p = jnp.dot(homeward, v, preferred_element_type=f32)
            send_x[h, :, t] = p.astype(bf).reshape(8, 16, 1024)
        for o in (4, 5, 2, 3, 6, 7, 1):
            zz, xx, cc = plane[o]
            push(("b", o, h), send_x.at[h, xx * 2 + cc], recv_b.at[h, j], device(zz, xx, cc))
        recv_b[h, j] = send_x[h, j]

    permute(0)
    permute(1)
    loads["gate"].wait()
    loads["up"].wait()
    loads["last"].wait()
    gather_own(0)
    for p in range(4):
        gather_on(p)
        if p > 0:
            hidden_on(p - 1)
        if p < 3:
            gather_own(p + 1)
        if p > 0:
            outputs(p - 1)
        hidden(p)
        if p == 3:
            homeward_x(0)
    hidden_on(3)
    outputs(3)
    homeward_x(1)
    for h in range(2):
        for o in plane_order:
            arrive(("b", o, h), recv_b.at[h, place_of(o)])

    def blended(t):
        w = blend[pl.ds(pl.multiple_of(t * 32, 32), 32), :]
        v = [recv_b[h, :, t // 2].reshape(128, 1024) for h in range(2)]
        v = jnp.concatenate(v + v, axis=0)
        return jnp.dot(w, v, preferred_element_type=f32).astype(bf)

    for way, t in (("O", over), ("R", right), ("L", left)):
        send_f[t] = blended(t)
        push(("f", way), send_f.at[t], fin.at[y], way_y[way])
    fin[y] = blended(y)
    for way, t in (("R", left), ("L", right), ("O", over)):
        arrive(("f", way), fin.at[t])
    square = jnp.zeros((32, 1), f32)
    for t in range(4):
        v = fin[t].astype(f32)
        square = square + jnp.sum(v * v, axis=1, keepdims=True)
    scale = lax.rsqrt(square * (1.0 / 4096) + 1e-6)
    for t in range(4):
        cols = slice(t * 1024, (t + 1) * 1024)
        out_ref[:, cols] = (stream_ref[:, cols].astype(f32) + fin[t].astype(f32) * scale * last_ref[:, cols]).astype(bf)
    for it in sends + down_copies + passed_on + copies + sent:
        it.wait_send()


def layer(*args):
    vm = pl.BlockSpec(memory_space=pltpu.VMEM)
    hbm = pl.BlockSpec(memory_space=pl.ANY)
    dma = pltpu.SemaphoreType.DMA
    bf, f32 = jnp.bfloat16, jnp.float32
    inputs = [((128, 512), bf), ((128, 128), bf), ((128, 128), bf)]
    late_inputs = [((32, 4096), bf), ((512, 4096), bf), ((1, 4096), f32), ((2, 128), jnp.int32), ((1, 128), f32),
                   ((4096, 256), bf), ((4096, 256), bf), ((1, 4096), f32)]
    sizes = [((32, 4096), bf), ((2, 8, 16, 2048), bf), ((4, 256, 1024), bf),
             ((2, 32, 128, 128), bf), ((2, 32, 128, 128), bf), ((512, 128), bf), ((KB, KB), bf), ((512, 128), f32),
             ((512, 128), f32), ((128, 512), bf), ((2, 128, 1024), bf), ((4, 2, 32, 2048), bf),
             ((2, 32, 2048), bf), ((2, 32, 2048), bf), ((2, 32, 2048), bf), ((2, 32, 2048), bf), ((2, 2, 128, 128), bf),
             ((2, 8, 16, 2048), bf), ((8, 16, 4096), bf), ((8, 4, 16, 4096), bf), ((4, 4, 128, 256), bf), ((8, 4, 16, 1024), bf),
             ((8, 4, 16, 1024), bf), ((2, 8, 2, 16, 1024), bf), ((2, 8, 2, 16, 1024), bf), ((128, 512), bf), ((4, 32, 1024), bf),
             ((4, 32, 1024), bf)]
    return pl.pallas_call(
        layer_kernel, out_shape=jax.ShapeDtypeStruct((32, 4096), bf), in_specs=[hbm] * 13, out_specs=vm,
        scratch_shapes=[pltpu.VMEM(*n) for n in inputs] + [pltpu.SMEM((1, 4), f32)] + [pltpu.VMEM(*n) for n in late_inputs + sizes]
        + [dma((126,)), dma((126,)), dma((6,)), dma((6,)), dma((6,)), dma((6,)), dma((112,)), dma((112,)), dma((13,))],
        compiler_params=pltpu.CompilerParams(collective_id=0, has_side_effects=True, vmem_limit_bytes=60 * 1024 * 1024),
    )(*args)


def on_device(
    queries, keys, values, break_bias, residual, w_out, ffn_gain, pick_ids, pair_logit, w_gate, w_up, w_down, out_gain
):
    return layer(
        queries, keys, values, break_bias.reshape(1, 4), residual, w_out, ffn_gain.reshape(1, -1), pick_ids.T,
        pair_logit.reshape(1, -1), w_gate[0], w_up[0], w_down[0], out_gain.reshape(1, -1)
    )


def solution(mesh):
    placed = (
        P("sp", "tp"),
        P("sp", "tp"),
        P("sp", "tp"),
        P("tp"),
        P(("sp", "tp"), None),
        P("tp", None),
        P(),
        P("sp", None),
        P("sp"),
        P("sp", None, "tp"),
        P("sp", None, "tp"),
        P("sp", "tp", None),
        P(),
    )
    return jax.shard_map(
        on_device, mesh=mesh, in_specs=placed, out_specs=P(("sp", "tp"), None), check_vma=False
    )
```

```python
import functools

import jax
import jax.numpy as jnp
from jax import lax
from jax.experimental import pallas as pl
from jax.experimental.pallas import tpu as pltpu
from jax.sharding import PartitionSpec as P

LOG2E = 1.4426950408889634
KB = 256

def attend_blocks(qs, k_ref, v_ref, tri, bias_ref, acc, used, pairs, shift=None, behind=False):
    rows = qs.shape[0] // 4
    c = LOG2E * 128 ** -0.5
    if shift is not None:
        col = lax.broadcasted_iota(jnp.int32, (rows, KB), 1)
        row = lax.broadcasted_iota(jnp.int32, (rows, KB), 0)
        before = col < row + shift
    keys = [jnp.concatenate([k_ref[0, p], k_ref[1, p]], axis=0) for p in pairs]
    vals = [jnp.concatenate([v_ref[0, p], v_ref[1, p]], axis=0) for p in pairs]
    scores = [lax.dot_general(qs[...], k, (((1,), (1,)), ((), ())), preferred_element_type=jnp.float32) for k in keys]
    zs, incls = [], []
    for s in scores:
        z_of, b_of = [], []
        for h in range(4):
            z = s[h * rows:(h + 1) * rows] * c + bias_ref[0, h] * LOG2E
            b = jnp.maximum(z, 0.0) + jnp.log2(1.0 + jnp.exp2(-jnp.abs(z)))
            if shift is not None:
                b = jnp.where(before, b, 0.0)
            z_of.append(z)
            b_of.append(b.astype(jnp.bfloat16))
        incls.append(jnp.dot(jnp.concatenate(b_of, axis=0), tri[...], preferred_element_type=jnp.float32))
        zs.append(z_of)
    gone = [jnp.zeros((rows, 128), jnp.float32) if behind else used[h * rows:(h + 1) * rows] for h in range(4)]
    total = None
    for z_of, incl, v in zip(zs, incls, vals):
        ws = []
        for h in range(4):
            sl = slice(h * rows, (h + 1) * rows)
            w = jnp.exp2(z_of[h] - incl[sl] - jnp.concatenate([gone[h], gone[h]], axis=1))
            if shift is not None:
                w = jnp.where(before, w, 0.0)
            ws.append(w.astype(jnp.bfloat16))
            gone[h] = gone[h] + jnp.broadcast_to(incl[sl, 0:1], (rows, 128))
        part = jnp.dot(jnp.concatenate(ws, axis=0), v, preferred_element_type=jnp.float32)
        total = part if total is None else total + part
    for h in range(4):
        sl = slice(h * rows, (h + 1) * rows)
        if behind:
            acc[sl] = total[sl] + jnp.exp2(-gone[h]) * acc[sl]
        else:
            acc[sl] += total[sl]
            used[sl] = gone[h]


MESH = pl.DeviceIdType.MESH
NZ, NX = 8, 4

def place():
    sp = lax.axis_index("sp")
    return sp // 8, (sp // 2) % 4, sp % 2

def device(z, x, c):
    return {"sp": z * 8 + x * 2 + c, "tp": lax.axis_index("tp")}

def gather_plan():
    zs = [("A", d) for d in (1, 2, 3, 4)] + [("B", d) for d in (1, 2, 3)]
    xs = [("A", 1), ("A", 2), ("B", 1)]
    none = ("O", 0)
    events = []
    for r in zs:
        events.append((r[1], "k", r, none, "z"))
    for rz in [none] + zs:
        for rx in xs:
            events.append((rz[1] + rx[1] + 0.25, "k", rz, rx, "x"))
    for r in xs:
        events.append((r[1], "v", none, r, "x"))
    for rx in [none] + xs:
        for rz in zs:
            events.append((rz[1] + rx[1] + 0.25, "v", rz, rx, "z"))
    return sorted(events)


def y_ring():
    y = lax.axis_index("tp")
    return y, (y + 1) % 4, (y + 3) % 4, (y + 2) % 4


OFFS = (0, -3, 3, 2, -2, 4, 1, -1)


def slot_columns(pick_ref, z):
    rows = lax.broadcasted_iota(jnp.int32, (128, 128), 0)
    lanes = lax.broadcasted_iota(jnp.int32, (128, 128), 1)
    earlier = (lanes < rows) & ((lanes & 96) == (rows & 96))
    across = [jnp.broadcast_to(pick_ref[k : k + 1, :], (128, 128)) for k in range(2)]
    wide = [w.astype(jnp.float32).T.astype(jnp.int32) for w in across]
    lane, late = [], []
    for w in wide:
        same = earlier & ((across[0] == w) | (across[1] == w))
        rank = jnp.sum(jnp.where(same, 1.0, 0.0), axis=1, keepdims=True).astype(jnp.int32)
        away = (z - (w >> 3)) & 7
        chunk = sum(jnp.where(away == (off & 7), o, 0) for o, off in enumerate(OFFS))
        lane.append((w & 7) * 16 + (chunk & 3) * 2 + rank)
        late.append(chunk >> 2)
    return lane, late


def layer_kernel(q_hbm, k_hbm, v_hbm, bias_hbm, res_hbm, w_hbm, gain_hbm, pick_hbm, logit_hbm, gate_hbm, up_hbm, down_ref, last_hbm,
                 out_ref,
                 q_ref, k_ref, v_ref, bias_ref, res_ref, w_ref, gain_ref, pick_ref, logit_ref, gate_ref, up_ref, last_ref,
                 stream_ref, disp_ref, down, kall, vall, qs, tri, acc, used, head, drelay, part, from_left, from_right, relay, summed, slots,
                 recv_x, send_z, got, hid, result, recv_r, send_x, recv_b, blend, send_f, fin, far,
                 ssem, rsem, dsend, drecv, msend, mrecv, xsend, xrecv, lsem):
    z, x, c = place()
    sp = lax.axis_index("sp")
    y, right, left, over = y_ring()
    sgn = 1 - 2 * c
    step = {"A": sgn, "B": -sgn, "O": 0}
    barrier = pltpu.get_barrier_semaphore()
    zn = {"A": (z + sgn + NZ) % NZ, "B": (z - sgn + NZ) % NZ}
    xn = {"A": (x + sgn + NX) % NX, "B": (x - sgn + NX) % NX}
    to_y = [{"sp": sp, "tp": t} for t in (right, left)]
    plane = [(z, (x + o // 2) % 4, (c + o) % 2) for o in range(8)]
    column = [((z + d) % 8, x, c) for d in range(8)]
    peers = [device(zn["A"], x, c), device(zn["B"], x, c), device(z, xn["A"], c), device(z, xn["B"], c), device(z, x, 1 - c)]
    for p in plane[1:] + column[1:]:
        pl.semaphore_signal(barrier, inc=1, device_id=device(*p), device_id_type=MESH)
    for t in (right, left, over):
        pl.semaphore_signal(barrier, inc=1, device_id={"sp": sp, "tp": t}, device_id_type=MESH)
    loads = {}
    for n, (name, src, dst) in enumerate((
        ("k", k_hbm, k_ref), ("v", v_hbm, v_ref), ("q", q_hbm, q_ref), ("bias", bias_hbm, bias_ref),
        ("picks", pick_hbm, pick_ref), ("w", w_hbm, w_ref), ("res", res_hbm, res_ref), ("gain", gain_hbm, gain_ref),
        ("gate", gate_hbm, gate_ref), ("up", up_hbm, up_ref), ("last", last_hbm, last_ref), ("logit", logit_hbm, logit_ref),
    )):
        loads[name] = pltpu.make_async_copy(src, dst, lsem.at[n + 1])
        loads[name].start()

    def columns(t):
        return pl.ds(pl.multiple_of(t * 1024, 1024), 1024)

    own_down = pltpu.make_async_copy(down_ref.at[:, columns(y)], down.at[y], lsem.at[0])
    own_down.start()
    loads["k"].wait()
    loads["v"].wait()
    pl.semaphore_wait(barrier, 17)

    def across(n, src, dst, to):
        return pltpu.make_async_remote_copy(src_ref=src, dst_ref=dst, send_sem=dsend.at[n], recv_sem=drecv.at[n], device_id=to_y[to], device_id_type=MESH)

    down_copies = [
        across(0, down_ref.at[0:128, columns(over)], drelay.at[0], 0),
        across(1, down_ref.at[128:256, columns(over)], drelay.at[1], 1),
        across(2, down_ref.at[:, columns(right)], down.at[y], 0),
        across(3, down_ref.at[:, columns(left)], down.at[y], 1),
    ]
    passed_on = [across(4, drelay.at[0], down.at[left, 0:128], 0), across(5, drelay.at[1], down.at[right, 128:256], 1)]
    down_arrivals = [
        across(2, down.at[left], down.at[left], 0), across(3, down.at[right], down.at[right], 1),
        across(4, down.at[over, 0:128], down.at[over, 0:128], 0), across(5, down.at[over, 128:256], down.at[over, 128:256], 1),
    ]
    zto = {"A": peers[0], "B": peers[1]}
    xto = {"A": peers[2], "B": peers[3]}
    full = {"k": kall, "v": vall}
    own = {"k": k_ref, "v": v_ref}
    tags = {}

    def tag(key):
        return tags.setdefault(key, len(tags))

    def source(rz, rx):
        return ((z - step[rz[0]] * rz[1] + NZ) % NZ) * NX + (x - step[rx[0]] * rx[1] + NX) % NX

    sends = []

    def send(arr, rz, rx, kind, to):
        i = source(rz, rx)
        src = own[arr] if (rz[1] == 0 and rx[1] == 0) else full[arr].at[c, i]
        if kind == "z":
            key, dst = (arr, (to, rz[1] + 1), rx, "z"), zto[to]
        elif kind == "x":
            key, dst = (arr, rz, (to, rx[1] + 1), "x"), xto[to]
        else:
            key, dst = (arr, rz, rx, "d"), peers[4]
        t = tag(key)
        copy = pltpu.make_async_remote_copy(src_ref=src, dst_ref=full[arr].at[c, i], send_sem=ssem.at[t], recv_sem=rsem.at[t], device_id=dst, device_id_type=MESH)
        copy.start()
        sends.append(copy)

    def arrived(arr, rz, rx, kind):
        t = tag((arr, rz, rx, kind))
        if kind == "d":
            i = ((z + step[rz[0]] * rz[1] + NZ) % NZ) * NX + (x + step[rx[0]] * rx[1] + NX) % NX
            ref = full[arr].at[1 - c, i]
        else:
            ref = full[arr].at[c, source(rz, rx)]
        pltpu.make_async_remote_copy(src_ref=ref, dst_ref=ref, send_sem=ssem.at[t], recv_sem=rsem.at[t], device_id=peers[4], device_id_type=MESH).wait_recv()

    most = {"A": 4, "B": 3}
    mostx = {"A": 2, "B": 1}
    o = ("O", 0)
    xs = [("A", 1), ("B", 1), ("A", 2)]
    send("k", o, o, "x", "A"); send("k", o, o, "x", "B"); send("v", o, o, "x", "A"); send("v", o, o, "x", "B")
    send("k", o, o, "d", None); send("v", o, o, "d", None)
    send("k", o, o, "z", "A"); send("k", o, o, "z", "B"); send("v", o, o, "z", "A"); send("v", o, o, "z", "B")
    me = z * NX + x
    kall[c, me] = k_ref[...]
    vall[c, me] = v_ref[...]
    loads["q"].wait()
    loads["bias"].wait()
    rows = q_ref.shape[0]
    for h in range(4):
        qs[h * rows:(h + 1) * rows] = q_ref[:, h * 128:(h + 1) * 128]
    r = lax.broadcasted_iota(jnp.int32, (KB, KB), 0)
    cc = lax.broadcasted_iota(jnp.int32, (KB, KB), 1)
    t = jnp.where(r >= cc, 1.0, 0.0).astype(jnp.bfloat16)
    tri[...] = t
    acc[...] = jnp.zeros_like(acc)
    used[...] = jnp.zeros_like(used)
    far[...] = jnp.zeros_like(far)
    for it in down_copies:
        it.start()

    def receive(arr, rz, rx, kind):
        arrived(arr, rz, rx, kind)
        if kind == "z" and rz[1] < most[rz[0]]:
            send(arr, rz, rx, "z", rz[0])
        if kind == "x" and rx[1] < mostx[rx[0]]:
            send(arr, rz, rx, "x", rx[0])
        if arr == "k" and kind == "z":
            send(arr, rz, rx, "x", "A"); send(arr, rz, rx, "x", "B")
        if arr == "v" and kind == "x":
            send(arr, rz, rx, "z", "A"); send(arr, rz, rx, "z", "B")
        send(arr, rz, rx, "d", None)

    def ways(d):
        return [o] if d == 0 else [("A", d), ("B", d)] if d < 4 else [("A", 4)]

    def settle(d):
        for arr in "kv":
            for rx in [o] + xs:
                for rz in ways(d):
                    arrived(arr, rz, rx, "d")

    def block(d, i):
        if d == 0 and i == 0:
            attend_blocks(qs, kall, vall, tri, bias_ref, acc, used, [me], c * rows)
        else:
            at = me - i if d == 0 else (z - d) * NX + 3 - i

            @pl.when(x >= i if d == 0 else z >= d)
            def _():
                attend_blocks(qs, kall, vall, tri, bias_ref, acc, used, [at] if d == 0 else [at, at - 1])

    def far_block(w, i):
        @pl.when(z >= 8 - w)
        def _():
            at = (z + w - 8) * NX + 1 + i
            attend_blocks(qs, kall, vall, tri, bias_ref, far, used, [at, at - 1], behind=True)

    waiting = []
    plan = gather_plan()
    for n, (when, arr, rz, rx, kind) in enumerate(plan):
        if n == 20:
            for way in (0, 1):
                down_copies[way].wait_recv()
                passed_on[way].start()
        receive(arr, rz, rx, kind)
        if waiting and n % 2 == 1:
            waiting.pop(0)()
        if n + 1 == len(plan) or plan[n + 1][0] > when:
            d = when - 2.25
            if d in (0, 1, 2, 3):
                waiting.append(functools.partial(settle, int(d)))
                waiting.extend(functools.partial(block, int(d), i) for i in (range(4) if d == 0 else (0, 2)))
                if d:
                    waiting.extend(functools.partial(far_block, int(d), i) for i in (0, 2))
    for step_of in waiting:
        step_of()
    settle(4)

    @pl.when(z >= 4)
    def _():
        attend_blocks(qs, kall, vall, tri, bias_ref, acc, used, [(z - 4) * NX + 3 - n for n in range(4)])

    acc[...] += jnp.exp2(-used[...]) * far[...]
    for h in range(4):
        a = acc[h * rows:(h + 1) * rows]
        sc = a * lax.rsqrt(jnp.mean(a * a, axis=-1, keepdims=True) + 1e-6)
        head[:, h * 128:(h + 1) * 128] = sc.astype(jnp.bfloat16)
    for it in down_arrivals:
        it.wait_recv()
    own_down.wait()
    loads["w"].wait()
    loads["res"].wait()
    loads["gain"].wait()
    loads["picks"].wait()
    def copy(n, src, dst, to):
        return pltpu.make_async_remote_copy(src_ref=src, dst_ref=dst, send_sem=msend.at[n], recv_sem=mrecv.at[n],
                                            device_id={"sp": sp, "tp": to}, device_id_type=MESH)

    def project(n):
        p = jnp.dot(head[...], w_ref[:, n * 1024:(n + 1) * 1024], preferred_element_type=jnp.float32).astype(jnp.bfloat16)
        for t in range(4):
            part[t, n // 2, :, (n % 2) * 1024:(n % 2 + 1) * 1024] = p[32 * t:32 * t + 32]

    copies = [
        copy(0, part.at[over, 0], relay.at[0], right),
        copy(1, part.at[over, 1], relay.at[1], left),
        copy(2, part.at[right, 1], from_left.at[1], right),
        copy(3, part.at[left, 0], from_right.at[0], left),
        copy(4, summed.at[0], from_left.at[0], right),
        copy(5, summed.at[1], from_right.at[1], left),
    ]
    project(0)
    project(1)
    copies[0].start()
    copies[3].start()
    project(2)
    project(3)
    copies[1].start()
    copies[2].start()
    lane, late = slot_columns(pick_ref, z)
    lanes = lax.broadcasted_iota(jnp.int32, (128, 128), 1)
    for h in range(2):
        for half in range(2):
            hit = [(lane[k] + 8 * half == lanes) & (late[k] == h) for k in range(2)]
            slots[h, half] = jnp.where(hit[0] | hit[1], 1.0, 0.0).astype(jnp.bfloat16)
    copies[0].wait_recv()
    summed[0] = (part[right, 0].astype(jnp.float32) + relay[0].astype(jnp.float32)).astype(jnp.bfloat16)
    copies[4].start()
    copies[1].wait_recv()
    summed[1] = (part[left, 1].astype(jnp.float32) + relay[1].astype(jnp.float32)).astype(jnp.bfloat16)
    copies[5].start()
    for n in (2, 3, 4, 5):
        copies[n].wait_recv()
    square = jnp.zeros((32, 1), jnp.float32)
    for h in range(2):
        cols = slice(h * 2048, (h + 1) * 2048)
        mixed = part[y, h].astype(jnp.float32) + from_left[h].astype(jnp.float32) + from_right[h].astype(jnp.float32)
        s = (res_ref[:, cols].astype(jnp.float32) + mixed).astype(jnp.bfloat16)
        stream_ref[:, cols] = s
        sf = s.astype(jnp.float32)
        square = square + jnp.sum(sf * sf, axis=1, keepdims=True)
    scale = lax.rsqrt(square * (1.0 / 4096) + 1e-6)
    tags_late = {}
    sent = []
    j = x * 2 + c
    bf, f32 = jnp.bfloat16, jnp.float32

    def late_copy(key, src, dst, to):
        n = tags_late.setdefault(key, len(tags_late))
        return pltpu.make_async_remote_copy(src_ref=src, dst_ref=dst, send_sem=xsend.at[n], recv_sem=xrecv.at[n],
                                            device_id=to, device_id_type=MESH)

    def push(key, src, dst, to):
        it = late_copy(key, src, dst, to)
        it.start()
        sent.append(it)

    def arrive(key, dst):
        late_copy(key, dst, dst, {"sp": sp, "tp": right}).wait_recv()

    way_y = {"R": {"sp": sp, "tp": right}, "L": {"sp": sp, "tp": left}, "O": {"sp": sp, "tp": over}}

    def pass_on_x(o, h):
        zz, xx, cc = plane[o]
        push(("x", o, h), disp_ref.at[h, xx * 2 + cc], recv_x.at[h, j], device(zz, xx, cc))

    own_rows = pl.ds(pl.multiple_of(y * 32, 32), 32)
    f = [(stream_ref[:, n * 2048:(n + 1) * 2048].astype(jnp.float32) * scale * gain_ref[:, n * 2048:(n + 1) * 2048]).astype(jnp.bfloat16) for n in range(2)]
    f = jnp.concatenate(f, axis=0)
    for h in range(2):
        mine = jnp.concatenate([slots[h, 0, own_rows, :], slots[h, 1, own_rows, :]], axis=0)
        d = lax.dot_general(mine, f, (((0,), (0,)), ((), ())), preferred_element_type=jnp.float32)
        disp_ref[h] = d.astype(jnp.bfloat16).reshape(8, 16, 2048)
        for o in (4, 5, 2, 3, 6, 7, 1):
            pass_on_x(o, h)
    loads["logit"].wait()
    logit = jnp.broadcast_to(logit_ref[...], (128, 128)).T
    second = ((lax.broadcasted_iota(jnp.int32, (128, 128), 0) >> 5) & 1) * 8
    chance = (jax.nn.sigmoid(logit), jax.nn.sigmoid(-logit))
    for h in range(2):
        w = sum(jnp.where((lane[k] + second == lanes) & (late[k] == h), chance[k], 0.0) for k in range(2))
        hi = w.astype(bf)
        blend[:, h * 128:(h + 1) * 128] = hi
        blend[:, 256 + h * 128:256 + (h + 1) * 128] = (w - hi.astype(f32)).astype(bf)
    a = lax.broadcasted_iota(jnp.int32, (128, 128), 0)
    b = lax.broadcasted_iota(jnp.int32, (128, 128), 1)
    outward = [jnp.where(b == ((a >> 1) & 7) * 16 + half * 8 + ((a >> 4) & 3) * 2 + (a & 1), 1.0, 0.0).astype(bf)[0:64] for half in range(2)]
    homeward = jnp.where(b == ((a >> 1) & 3) * 32 + ((a >> 3) & 1) * 16 + (a >> 4) * 2 + (a & 1), 1.0, 0.0).astype(bf)
    halves = [slice(0, 2048), slice(2048, 4096)]
    plane_order = (1, 2, 3, 6, 7, 4, 5)

    def place_of(o):
        return ((x - o // 2 + 4) % 4) * 2 + (c + o) % 2

    def over_y(o):
        for half in range(2):
            part = got.at[o, y, :, halves[half]]
            for way in "RL":
                push(("g", way, o, half), part, part, way_y[way])

    def permute(h):
        recv_x[h, j] = disp_ref[h, j]
        for o in plane_order:
            arrive(("x", o, h), recv_x.at[h, place_of(o)])
        v = recv_x[h].reshape(128, 2048)
        for half in range(2):
            p = jnp.dot(outward[half], v, preferred_element_type=f32).astype(bf).reshape(4, 16, 2048)
            send_z[4 * h:4 * h + 4, :, halves[half]] = p
            if h == 0:
                got[0, y, :, halves[half]] = p[0]
        for o in range(4 * h, 4 * h + 4):
            if o:
                push(("z", o), send_z.at[o], got.at[o, y], device((z - OFFS[o] + 8) % 8, x, c))
            else:
                over_y(0)

    def gather_own(g):
        for o in (2 * g, 2 * g + 1):
            if o:
                arrive(("z", o), got.at[o, y])
                over_y(o)

    def gather_on(g):
        for o in (2 * g, 2 * g + 1):
            for h, way, t in ((0, "R", left), (1, "L", right)):
                part = got.at[o, t, :, halves[h]]
                arrive(("g", way, o, h), part)
                push(("h", way, o), part, part, way_y[way])

    def hidden(g):
        for o in (2 * g, 2 * g + 1):
            arrive(("g", "R", o, 1), got.at[o, left, :, halves[1]])
            arrive(("g", "L", o, 0), got.at[o, right, :, halves[0]])
            arrive(("h", "R", o), got.at[o, over, :, halves[0]])
            arrive(("h", "L", o), got.at[o, over, :, halves[1]])
        v = got[2 * g:2 * g + 2].reshape(128, 4096)
        gate = jnp.dot(v, gate_ref[...], preferred_element_type=f32)
        up = jnp.dot(v, up_ref[...], preferred_element_type=f32)
        hid[g, y] = (gate / (1.0 + jnp.exp(-gate)) * up).astype(bf)
        for way in "RL":
            push(("u", way, g), hid.at[g, y], hid.at[g, y], way_y[way])

    def hidden_on(g):
        arrive(("u", "R", g), hid.at[g, left])
        half = hid.at[g, left, 0:64]
        push(("v", "R", g), half, half, way_y["R"])
        arrive(("u", "L", g), hid.at[g, right])
        half = hid.at[g, right, 64:128]
        push(("v", "L", g), half, half, way_y["L"])

    def outputs(g):
        arrive(("v", "R", g), hid.at[g, over, 0:64])
        arrive(("v", "L", g), hid.at[g, over, 64:128])
        h = jnp.concatenate([hid[g, t] for t in range(4)], axis=1)
        r = jnp.dot(h, down[...].reshape(1024, 1024), preferred_element_type=f32)
        result[2 * g:2 * g + 2] = r.astype(bf).reshape(2, 4, 16, 1024)
        for o in (2 * g, 2 * g + 1):
            if o:
                push(("r", o), result.at[o], recv_r.at[o], device((z + OFFS[o] + 8) % 8, x, c))
            else:
                recv_r[0] = result[0]

    def homeward_x(h):
        for o in range(4 * h, 4 * h + 4):
            if o:
                arrive(("r", o), recv_r.at[o])
        for t in range(2):
            v = recv_r[4 * h:4 * h + 4, 2 * t:2 * t + 2].reshape(128, 1024)
            p = jnp.dot(homeward, v, preferred_element_type=f32)
            send_x[h, :, t] = p.astype(bf).reshape(8, 16, 1024)
        for o in (4, 5, 2, 3, 6, 7, 1):
            zz, xx, cc = plane[o]
            push(("b", o, h), send_x.at[h, xx * 2 + cc], recv_b.at[h, j], device(zz, xx, cc))
        recv_b[h, j] = send_x[h, j]

    permute(0)
    permute(1)
    loads["gate"].wait()
    loads["up"].wait()
    loads["last"].wait()
    gather_own(0)
    for p in range(4):
        gather_on(p)
        if p > 0:
            hidden_on(p - 1)
        if p < 3:
            gather_own(p + 1)
        hidden(p)
        if p > 0:
            outputs(p - 1)
    hidden_on(3)
    homeward_x(0)
    outputs(3)
    homeward_x(1)
    for h in range(2):
        for o in plane_order:
            arrive(("b", o, h), recv_b.at[h, place_of(o)])

    def blended(t):
        w = blend[pl.ds(pl.multiple_of(t * 32, 32), 32), :]
        v = [recv_b[h, :, t // 2].reshape(128, 1024) for h in range(2)]
        v = jnp.concatenate(v + v, axis=0)
        return jnp.dot(w, v, preferred_element_type=f32).astype(bf)

    for way, t in (("O", over), ("R", right), ("L", left)):
        send_f[t] = blended(t)
        push(("f", way), send_f.at[t], fin.at[y], way_y[way])
    fin[y] = blended(y)
    for way, t in (("R", left), ("L", right), ("O", over)):
        arrive(("f", way), fin.at[t])
    square = jnp.zeros((32, 1), f32)
    for t in range(4):
        v = fin[t].astype(f32)
        square = square + jnp.sum(v * v, axis=1, keepdims=True)
    scale = lax.rsqrt(square * (1.0 / 4096) + 1e-6)
    for t in range(4):
        cols = slice(t * 1024, (t + 1) * 1024)
        out_ref[:, cols] = (stream_ref[:, cols].astype(f32) + fin[t].astype(f32) * scale * last_ref[:, cols]).astype(bf)
    for it in sends + down_copies + passed_on + copies + sent:
        it.wait_send()


def layer(*args):
    vm = pl.BlockSpec(memory_space=pltpu.VMEM)
    hbm = pl.BlockSpec(memory_space=pl.ANY)
    dma = pltpu.SemaphoreType.DMA
    bf, f32 = jnp.bfloat16, jnp.float32
    inputs = [((128, 512), bf), ((128, 128), bf), ((128, 128), bf)]
    late_inputs = [((32, 4096), bf), ((512, 4096), bf), ((1, 4096), f32), ((2, 128), jnp.int32), ((1, 128), f32),
                   ((4096, 256), bf), ((4096, 256), bf), ((1, 4096), f32)]
    sizes = [((32, 4096), bf), ((2, 8, 16, 2048), bf), ((4, 256, 1024), bf),
             ((2, 32, 128, 128), bf), ((2, 32, 128, 128), bf), ((512, 128), bf), ((KB, KB), bf), ((512, 128), f32),
             ((512, 128), f32), ((128, 512), bf), ((2, 128, 1024), bf), ((4, 2, 32, 2048), bf),
             ((2, 32, 2048), bf), ((2, 32, 2048), bf), ((2, 32, 2048), bf), ((2, 32, 2048), bf), ((2, 2, 128, 128), bf),
             ((2, 8, 16, 2048), bf), ((8, 16, 4096), bf), ((8, 4, 16, 4096), bf), ((4, 4, 128, 256), bf), ((8, 4, 16, 1024), bf),
             ((8, 4, 16, 1024), bf), ((2, 8, 2, 16, 1024), bf), ((2, 8, 2, 16, 1024), bf), ((128, 512), bf), ((4, 32, 1024), bf),
             ((4, 32, 1024), bf), ((512, 128), f32)]
    return pl.pallas_call(
        layer_kernel, out_shape=jax.ShapeDtypeStruct((32, 4096), bf), in_specs=[hbm] * 13, out_specs=vm,
        scratch_shapes=[pltpu.VMEM(*n) for n in inputs] + [pltpu.SMEM((1, 4), f32)] + [pltpu.VMEM(*n) for n in late_inputs + sizes]
        + [dma((126,)), dma((126,)), dma((6,)), dma((6,)), dma((6,)), dma((6,)), dma((112,)), dma((112,)), dma((13,))],
        compiler_params=pltpu.CompilerParams(collective_id=0, has_side_effects=True, vmem_limit_bytes=60 * 1024 * 1024),
    )(*args)


def on_device(
    queries, keys, values, break_bias, residual, w_out, ffn_gain, pick_ids, pair_logit, w_gate, w_up, w_down, out_gain
):
    return layer(
        queries, keys, values, break_bias.reshape(1, 4), residual, w_out, ffn_gain.reshape(1, -1), pick_ids.T,
        pair_logit.reshape(1, -1), w_gate[0], w_up[0], w_down[0], out_gain.reshape(1, -1)
    )


def solution(mesh):
    placed = (
        P("sp", "tp"),
        P("sp", "tp"),
        P("sp", "tp"),
        P("tp"),
        P(("sp", "tp"), None),
        P("tp", None),
        P(),
        P("sp", None),
        P("sp"),
        P("sp", None, "tp"),
        P("sp", None, "tp"),
        P("sp", "tp", None),
        P(),
    )
    return jax.shard_map(
        on_device, mesh=mesh, in_specs=placed, out_specs=P(("sp", "tp"), None), check_vma=False
    )
```

```python
import functools

import jax
import jax.numpy as jnp
from jax import lax
from jax.experimental import pallas as pl
from jax.experimental.pallas import tpu as pltpu
from jax.sharding import PartitionSpec as P

LOG2E = 1.4426950408889634
KB = 256

def attend_blocks(qs, k_ref, v_ref, tri, bias_ref, acc, used, pairs, shift=None, behind=False):
    rows = qs.shape[0] // 4
    c = LOG2E * 128 ** -0.5
    if shift is not None:
        col = lax.broadcasted_iota(jnp.int32, (rows, KB), 1)
        row = lax.broadcasted_iota(jnp.int32, (rows, KB), 0)
        before = col < row + shift
    keys = [jnp.concatenate([k_ref[0, p], k_ref[1, p]], axis=0) for p in pairs]
    vals = [jnp.concatenate([v_ref[0, p], v_ref[1, p]], axis=0) for p in pairs]
    scores = [lax.dot_general(qs[...], k, (((1,), (1,)), ((), ())), preferred_element_type=jnp.float32) for k in keys]
    zs, incls = [], []
    for s in scores:
        z_of, b_of = [], []
        for h in range(4):
            z = s[h * rows:(h + 1) * rows] * c + bias_ref[0, h] * LOG2E
            b = jnp.maximum(z, 0.0) + jnp.log2(1.0 + jnp.exp2(-jnp.abs(z)))
            if shift is not None:
                b = jnp.where(before, b, 0.0)
            z_of.append(z)
            b_of.append(b.astype(jnp.bfloat16))
        incls.append(jnp.dot(jnp.concatenate(b_of, axis=0), tri[...], preferred_element_type=jnp.float32))
        zs.append(z_of)
    gone = [jnp.zeros((rows, 128), jnp.float32) if behind else used[h * rows:(h + 1) * rows] for h in range(4)]
    total = None
    for z_of, incl, v in zip(zs, incls, vals):
        ws = []
        for h in range(4):
            sl = slice(h * rows, (h + 1) * rows)
            w = jnp.exp2(z_of[h] - incl[sl] - jnp.concatenate([gone[h], gone[h]], axis=1))
            if shift is not None:
                w = jnp.where(before, w, 0.0)
            ws.append(w.astype(jnp.bfloat16))
            gone[h] = gone[h] + jnp.broadcast_to(incl[sl, 0:1], (rows, 128))
        part = jnp.dot(jnp.concatenate(ws, axis=0), v, preferred_element_type=jnp.float32)
        total = part if total is None else total + part
    for h in range(4):
        sl = slice(h * rows, (h + 1) * rows)
        if behind:
            acc[sl] = total[sl] + jnp.exp2(-gone[h]) * acc[sl]
        else:
            acc[sl] += total[sl]
            used[sl] = gone[h]


MESH = pl.DeviceIdType.MESH
NZ, NX = 8, 4

def place():
    sp = lax.axis_index("sp")
    return sp // 8, (sp // 2) % 4, sp % 2

def device(z, x, c):
    return {"sp": z * 8 + x * 2 + c, "tp": lax.axis_index("tp")}

def gather_plan():
    zs = [("A", d) for d in (1, 2, 3, 4)] + [("B", d) for d in (1, 2, 3)]
    xs = [("A", 1), ("A", 2), ("B", 1)]
    none = ("O", 0)
    events = []
    for r in zs:
        events.append((r[1], "k", r, none, "z"))
    for rz in [none] + zs:
        for rx in xs:
            events.append((rz[1] + rx[1] + 0.25, "k", rz, rx, "x"))
    for r in xs:
        events.append((r[1], "v", none, r, "x"))
    for rx in [none] + xs:
        for rz in zs:
            events.append((rz[1] + rx[1] + 0.25, "v", rz, rx, "z"))
    return sorted(events)


def y_ring():
    y = lax.axis_index("tp")
    return y, (y + 1) % 4, (y + 3) % 4, (y + 2) % 4


OFFS = (0, 3, -3, 2, -2, 4, 1, -1)


def slot_columns(pick_ref, z):
    rows = lax.broadcasted_iota(jnp.int32, (128, 128), 0)
    lanes = lax.broadcasted_iota(jnp.int32, (128, 128), 1)
    earlier = (lanes < rows) & ((lanes & 96) == (rows & 96))
    across = [jnp.broadcast_to(pick_ref[k : k + 1, :], (128, 128)) for k in range(2)]
    wide = [w.astype(jnp.float32).T.astype(jnp.int32) for w in across]
    place, chunks = [], []
    for w in wide:
        same = earlier & ((across[0] == w) | (across[1] == w))
        rank = jnp.sum(jnp.where(same, 1.0, 0.0), axis=1, keepdims=True).astype(jnp.int32)
        away = (z - (w >> 3)) & 7
        chunk = sum(jnp.where(away == (off & 7), o, 0) for o, off in enumerate(OFFS))
        place.append((w & 7) * 16 + rank)
        chunks.append(chunk)
    return place, chunks


def layer_kernel(q_hbm, k_hbm, v_hbm, bias_hbm, res_hbm, w_hbm, gain_hbm, pick_hbm, logit_hbm, gate_hbm, up_hbm, down_ref, last_hbm,
                 out_ref,
                 q_ref, k_ref, v_ref, bias_ref, res_ref, w_ref, gain_ref, pick_ref, logit_ref, gate_ref, up_ref, last_ref,
                 stream_ref, disp_ref, down, kall, vall, qs, tri, acc, used, head, drelay, part, from_left, from_right, relay, summed, slots,
                 recv_x, send_z, got, hid, result, recv_r, send_x, recv_b, blend, send_f, fin, far,
                 ssem, rsem, dsend, drecv, msend, mrecv, xsend, xrecv, lsem):
    z, x, c = place()
    sp = lax.axis_index("sp")
    y, right, left, over = y_ring()
    sgn = 1 - 2 * c
    step = {"A": sgn, "B": -sgn, "O": 0}
    barrier = pltpu.get_barrier_semaphore()
    zn = {"A": (z + sgn + NZ) % NZ, "B": (z - sgn + NZ) % NZ}
    xn = {"A": (x + sgn + NX) % NX, "B": (x - sgn + NX) % NX}
    to_y = [{"sp": sp, "tp": t} for t in (right, left)]
    plane = [(z, (x + o // 2) % 4, (c + o) % 2) for o in range(8)]
    column = [((z + d) % 8, x, c) for d in range(8)]
    peers = [device(zn["A"], x, c), device(zn["B"], x, c), device(z, xn["A"], c), device(z, xn["B"], c), device(z, x, 1 - c)]
    for p in plane[1:] + column[1:]:
        pl.semaphore_signal(barrier, inc=1, device_id=device(*p), device_id_type=MESH)
    for t in (right, left, over):
        pl.semaphore_signal(barrier, inc=1, device_id={"sp": sp, "tp": t}, device_id_type=MESH)
    loads = {}
    for n, (name, src, dst) in enumerate((
        ("k", k_hbm, k_ref), ("v", v_hbm, v_ref), ("q", q_hbm, q_ref), ("bias", bias_hbm, bias_ref),
        ("picks", pick_hbm, pick_ref), ("w", w_hbm, w_ref), ("res", res_hbm, res_ref), ("gain", gain_hbm, gain_ref),
        ("gate", gate_hbm, gate_ref), ("up", up_hbm, up_ref), ("last", last_hbm, last_ref), ("logit", logit_hbm, logit_ref),
    )):
        loads[name] = pltpu.make_async_copy(src, dst, lsem.at[n + 1])
        loads[name].start()

    def columns(t):
        return pl.ds(pl.multiple_of(t * 1024, 1024), 1024)

    own_down = pltpu.make_async_copy(down_ref.at[:, columns(y)], down.at[y], lsem.at[0])
    own_down.start()
    loads["k"].wait()
    loads["v"].wait()
    pl.semaphore_wait(barrier, 17)

    def across(n, src, dst, to):
        return pltpu.make_async_remote_copy(src_ref=src, dst_ref=dst, send_sem=dsend.at[n], recv_sem=drecv.at[n], device_id=to_y[to], device_id_type=MESH)

    down_copies = [
        across(0, down_ref.at[0:128, columns(over)], drelay.at[0], 0),
        across(1, down_ref.at[128:256, columns(over)], drelay.at[1], 1),
        across(2, down_ref.at[:, columns(right)], down.at[y], 0),
        across(3, down_ref.at[:, columns(left)], down.at[y], 1),
    ]
    passed_on = [across(4, drelay.at[0], down.at[left, 0:128], 0), across(5, drelay.at[1], down.at[right, 128:256], 1)]
    down_arrivals = [
        across(2, down.at[left], down.at[left], 0), across(3, down.at[right], down.at[right], 1),
        across(4, down.at[over, 0:128], down.at[over, 0:128], 0), across(5, down.at[over, 128:256], down.at[over, 128:256], 1),
    ]
    zto = {"A": peers[0], "B": peers[1]}
    xto = {"A": peers[2], "B": peers[3]}
    full = {"k": kall, "v": vall}
    own = {"k": k_ref, "v": v_ref}
    tags = {}

    def tag(key):
        return tags.setdefault(key, len(tags))

    def source(rz, rx):
        return ((z - step[rz[0]] * rz[1] + NZ) % NZ) * NX + (x - step[rx[0]] * rx[1] + NX) % NX

    sends = []

    def send(arr, rz, rx, kind, to):
        i = source(rz, rx)
        src = own[arr] if (rz[1] == 0 and rx[1] == 0) else full[arr].at[c, i]
        if kind == "z":
            key, dst = (arr, (to, rz[1] + 1), rx, "z"), zto[to]
        elif kind == "x":
            key, dst = (arr, rz, (to, rx[1] + 1), "x"), xto[to]
        else:
            key, dst = (arr, rz, rx, "d"), peers[4]
        t = tag(key)
        copy = pltpu.make_async_remote_copy(src_ref=src, dst_ref=full[arr].at[c, i], send_sem=ssem.at[t], recv_sem=rsem.at[t], device_id=dst, device_id_type=MESH)
        copy.start()
        sends.append(copy)

    def arrived(arr, rz, rx, kind):
        t = tag((arr, rz, rx, kind))
        if kind == "d":
            i = ((z + step[rz[0]] * rz[1] + NZ) % NZ) * NX + (x + step[rx[0]] * rx[1] + NX) % NX
            ref = full[arr].at[1 - c, i]
        else:
            ref = full[arr].at[c, source(rz, rx)]
        pltpu.make_async_remote_copy(src_ref=ref, dst_ref=ref, send_sem=ssem.at[t], recv_sem=rsem.at[t], device_id=peers[4], device_id_type=MESH).wait_recv()

    most = {"A": 4, "B": 3}
    mostx = {"A": 2, "B": 1}
    o = ("O", 0)
    xs = [("A", 1), ("B", 1), ("A", 2)]
    send("k", o, o, "x", "A"); send("k", o, o, "x", "B"); send("v", o, o, "x", "A"); send("v", o, o, "x", "B")
    send("k", o, o, "d", None); send("v", o, o, "d", None)
    send("k", o, o, "z", "A"); send("k", o, o, "z", "B"); send("v", o, o, "z", "A"); send("v", o, o, "z", "B")
    me = z * NX + x
    kall[c, me] = k_ref[...]
    vall[c, me] = v_ref[...]
    loads["q"].wait()
    loads["bias"].wait()
    rows = q_ref.shape[0]
    for h in range(4):
        qs[h * rows:(h + 1) * rows] = q_ref[:, h * 128:(h + 1) * 128]
    r = lax.broadcasted_iota(jnp.int32, (KB, KB), 0)
    cc = lax.broadcasted_iota(jnp.int32, (KB, KB), 1)
    t = jnp.where(r >= cc, 1.0, 0.0).astype(jnp.bfloat16)
    tri[...] = t
    acc[...] = jnp.zeros_like(acc)
    used[...] = jnp.zeros_like(used)
    far[...] = jnp.zeros_like(far)
    for it in down_copies:
        it.start()

    def receive(arr, rz, rx, kind):
        arrived(arr, rz, rx, kind)
        if kind == "z" and rz[1] < most[rz[0]]:
            send(arr, rz, rx, "z", rz[0])
        if kind == "x" and rx[1] < mostx[rx[0]]:
            send(arr, rz, rx, "x", rx[0])
        if arr == "k" and kind == "z":
            send(arr, rz, rx, "x", "A"); send(arr, rz, rx, "x", "B")
        if arr == "v" and kind == "x":
            send(arr, rz, rx, "z", "A"); send(arr, rz, rx, "z", "B")
        send(arr, rz, rx, "d", None)

    def ways(d):
        return [o] if d == 0 else [("A", d), ("B", d)] if d < 4 else [("A", 4)]

    def settle(d):
        for arr in "kv":
            for rx in [o] + xs:
                for rz in ways(d):
                    arrived(arr, rz, rx, "d")

    def block(d, i):
        if d == 0 and i == 0:
            attend_blocks(qs, kall, vall, tri, bias_ref, acc, used, [me], c * rows)
        else:
            at = me - i if d == 0 else (z - d) * NX + 3 - i

            @pl.when(x >= i if d == 0 else z >= d)
            def _():
                attend_blocks(qs, kall, vall, tri, bias_ref, acc, used, [at] if d == 0 else [at, at - 1])

    def far_block(w, i):
        @pl.when(z >= 8 - w)
        def _():
            at = (z + w - 8) * NX + 1 + i
            attend_blocks(qs, kall, vall, tri, bias_ref, far, used, [at, at - 1], behind=True)

    waiting = []
    plan = gather_plan()
    for n, (when, arr, rz, rx, kind) in enumerate(plan):
        if n == 20:
            for way in (0, 1):
                down_copies[way].wait_recv()
                passed_on[way].start()
        receive(arr, rz, rx, kind)
        if waiting and n % 2 == 1:
            waiting.pop(0)()
        if n + 1 == len(plan) or plan[n + 1][0] > when:
            d = when - 2.25
            if d in (0, 1, 2, 3):
                waiting.append(functools.partial(settle, int(d)))
                waiting.extend(functools.partial(block, int(d), i) for i in (range(4) if d == 0 else (0, 2)))
                if d:
                    waiting.extend(functools.partial(far_block, int(d), i) for i in (0, 2))
    for step_of in waiting:
        step_of()
    settle(4)

    @pl.when(z >= 4)
    def _():
        attend_blocks(qs, kall, vall, tri, bias_ref, acc, used, [(z - 4) * NX + 3 - n for n in range(4)])

    acc[...] += jnp.exp2(-used[...]) * far[...]
    for h in range(4):
        a = acc[h * rows:(h + 1) * rows]
        sc = a * lax.rsqrt(jnp.mean(a * a, axis=-1, keepdims=True) + 1e-6)
        head[:, h * 128:(h + 1) * 128] = sc.astype(jnp.bfloat16)
    for it in down_arrivals:
        it.wait_recv()
    own_down.wait()
    loads["w"].wait()
    loads["res"].wait()
    loads["gain"].wait()
    loads["picks"].wait()
    def copy(n, src, dst, to):
        return pltpu.make_async_remote_copy(src_ref=src, dst_ref=dst, send_sem=msend.at[n], recv_sem=mrecv.at[n],
                                            device_id={"sp": sp, "tp": to}, device_id_type=MESH)

    def project(n):
        p = jnp.dot(head[...], w_ref[:, n * 1024:(n + 1) * 1024], preferred_element_type=jnp.float32).astype(jnp.bfloat16)
        for t in range(4):
            part[t, n // 2, :, (n % 2) * 1024:(n % 2 + 1) * 1024] = p[32 * t:32 * t + 32]

    copies = [
        copy(0, part.at[over, 0], relay.at[0], right),
        copy(1, part.at[over, 1], relay.at[1], left),
        copy(2, part.at[right, 1], from_left.at[1], right),
        copy(3, part.at[left, 0], from_right.at[0], left),
        copy(4, summed.at[0], from_left.at[0], right),
        copy(5, summed.at[1], from_right.at[1], left),
    ]
    project(0)
    project(1)
    copies[0].start()
    copies[3].start()
    project(2)
    project(3)
    copies[1].start()
    copies[2].start()
    spot, chunks = slot_columns(pick_ref, z)
    lanes = lax.broadcasted_iota(jnp.int32, (128, 128), 1)
    for g in range(4):
        for n in range(4):
            hit = [(spot[k] + (chunks[k] & 1) * 2 + 4 * n == lanes) & ((chunks[k] >> 1) == g) for k in range(2)]
            slots[g, n] = jnp.where(hit[0] | hit[1], 1.0, 0.0).astype(jnp.bfloat16)
    copies[0].wait_recv()
    summed[0] = (part[right, 0].astype(jnp.float32) + relay[0].astype(jnp.float32)).astype(jnp.bfloat16)
    copies[4].start()
    copies[1].wait_recv()
    summed[1] = (part[left, 1].astype(jnp.float32) + relay[1].astype(jnp.float32)).astype(jnp.bfloat16)
    copies[5].start()
    for n in (2, 3, 4, 5):
        copies[n].wait_recv()
    square = jnp.zeros((32, 1), jnp.float32)
    for h in range(2):
        cols = slice(h * 2048, (h + 1) * 2048)
        mixed = part[y, h].astype(jnp.float32) + from_left[h].astype(jnp.float32) + from_right[h].astype(jnp.float32)
        s = (res_ref[:, cols].astype(jnp.float32) + mixed).astype(jnp.bfloat16)
        stream_ref[:, cols] = s
        sf = s.astype(jnp.float32)
        square = square + jnp.sum(sf * sf, axis=1, keepdims=True)
    scale = lax.rsqrt(square * (1.0 / 4096) + 1e-6)
    tags_late = {}
    sent = []
    j = x * 2 + c
    bf, f32 = jnp.bfloat16, jnp.float32

    def late_copy(key, src, dst, to):
        n = tags_late.setdefault(key, len(tags_late))
        return pltpu.make_async_remote_copy(src_ref=src, dst_ref=dst, send_sem=xsend.at[n], recv_sem=xrecv.at[n],
                                            device_id=to, device_id_type=MESH)

    def push(key, src, dst, to):
        it = late_copy(key, src, dst, to)
        it.start()
        sent.append(it)

    def arrive(key, dst):
        late_copy(key, dst, dst, {"sp": sp, "tp": right}).wait_recv()

    way_y = {"R": {"sp": sp, "tp": right}, "L": {"sp": sp, "tp": left}, "O": {"sp": sp, "tp": over}}

    def pass_on_x(o, g):
        zz, xx, cc = plane[o]
        push(("x", o, g), disp_ref.at[g, xx * 2 + cc], recv_x.at[g, j], device(zz, xx, cc))

    own_rows = pl.ds(pl.multiple_of(y * 32, 32), 32)
    quarters = [slice(n * 1024, (n + 1) * 1024) for n in range(4)]
    f = [(stream_ref[:, cols].astype(jnp.float32) * scale * gain_ref[:, cols]).astype(jnp.bfloat16) for cols in quarters]
    f = jnp.concatenate(f, axis=0)
    for g in range(4):
        mine = jnp.concatenate([slots[g, n, own_rows, :] for n in range(4)], axis=0)
        d = lax.dot_general(mine, f, (((0,), (0,)), ((), ())), preferred_element_type=jnp.float32)
        disp_ref[g] = d.astype(jnp.bfloat16).reshape(8, 16, 1024)
        for o in (4, 5, 2, 3, 6, 7, 1):
            pass_on_x(o, g)
    loads["logit"].wait()
    logit = jnp.broadcast_to(logit_ref[...], (128, 128)).T
    block_of = ((lax.broadcasted_iota(jnp.int32, (128, 128), 0) >> 5) & 3) * 4
    chance = (jax.nn.sigmoid(logit), jax.nn.sigmoid(-logit))
    for g in range(4):
        w = sum(jnp.where((spot[k] + (chunks[k] & 1) * 2 + block_of == lanes) & ((chunks[k] >> 1) == g), chance[k], 0.0) for k in range(2))
        hi = w.astype(bf)
        blend[:, g * 128:(g + 1) * 128] = hi
        blend[:, 512 + g * 128:512 + (g + 1) * 128] = (w - hi.astype(f32)).astype(bf)
    a = lax.broadcasted_iota(jnp.int32, (128, 128), 0)
    b = lax.broadcasted_iota(jnp.int32, (128, 128), 1)
    outward = [jnp.where(b == ((a >> 1) & 7) * 16 + n * 4 + ((a >> 4) & 1) * 2 + (a & 1), 1.0, 0.0).astype(bf)[0:32] for n in range(4)]
    homeward = jnp.where(b == ((a >> 1) & 1) * 64 + ((a >> 2) & 3) * 16 + (a >> 4) * 2 + (a & 1), 1.0, 0.0).astype(bf)
    halves = [slice(0, 2048), slice(2048, 4096)]
    plane_order = (1, 2, 3, 6, 7, 4, 5)

    def place_of(o):
        return ((x - o // 2 + 4) % 4) * 2 + (c + o) % 2

    def over_y(o):
        for half in range(2):
            part = got.at[o, y, :, halves[half]]
            for way in "RL":
                push(("g", way, o, half), part, part, way_y[way])

    def permute(g):
        recv_x[g, j] = disp_ref[g, j]
        for o in plane_order:
            arrive(("x", o, g), recv_x.at[g, place_of(o)])
        v = recv_x[g].reshape(128, 1024)
        for n in range(4):
            p = jnp.dot(outward[n], v, preferred_element_type=f32).astype(bf).reshape(2, 16, 1024)
            send_z[2 * g:2 * g + 2, :, quarters[n]] = p
            if g == 0:
                got[0, y, :, quarters[n]] = p[0]
        for o in (2 * g, 2 * g + 1):
            if o:
                push(("z", o), send_z.at[o], got.at[o, y], device((z - OFFS[o] + 8) % 8, x, c))
            else:
                over_y(0)

    def own(o):
        arrive(("z", o), got.at[o, y])
        over_y(o)

    def on(o):
        for h, way, t in ((0, "R", left), (1, "L", right)):
            part = got.at[o, t, :, halves[h]]
            arrive(("g", way, o, h), part)
            push(("h", way, o), part, part, way_y[way])

    def gather_own(g):
        own(2 * g)
        own(2 * g + 1)

    def gather_on(g):
        on(2 * g)
        on(2 * g + 1)

    def hidden(g):
        for o in (2 * g, 2 * g + 1):
            arrive(("g", "R", o, 1), got.at[o, left, :, halves[1]])
            arrive(("g", "L", o, 0), got.at[o, right, :, halves[0]])
            arrive(("h", "R", o), got.at[o, over, :, halves[0]])
            arrive(("h", "L", o), got.at[o, over, :, halves[1]])
        v = got[2 * g:2 * g + 2].reshape(128, 4096)
        gate = jnp.dot(v, gate_ref[...], preferred_element_type=f32)
        up = jnp.dot(v, up_ref[...], preferred_element_type=f32)
        hid[g, y] = (gate / (1.0 + jnp.exp(-gate)) * up).astype(bf)
        for way in "RL":
            push(("u", way, g), hid.at[g, y], hid.at[g, y], way_y[way])

    def hidden_on(g):
        arrive(("u", "R", g), hid.at[g, left])
        half = hid.at[g, left, 0:64]
        push(("v", "R", g), half, half, way_y["R"])
        arrive(("u", "L", g), hid.at[g, right])
        half = hid.at[g, right, 64:128]
        push(("v", "L", g), half, half, way_y["L"])

    def outputs(g):
        arrive(("v", "R", g), hid.at[g, over, 0:64])
        arrive(("v", "L", g), hid.at[g, over, 64:128])
        h = jnp.concatenate([hid[g, t] for t in range(4)], axis=1)
        r = jnp.dot(h, down[...].reshape(1024, 1024), preferred_element_type=f32)
        result[2 * g:2 * g + 2] = r.astype(bf).reshape(2, 4, 16, 1024)
        for o in (2 * g, 2 * g + 1):
            if o:
                push(("r", o), result.at[o], recv_r.at[o], device((z + OFFS[o] + 8) % 8, x, c))
            else:
                recv_r[0] = result[0]

    def homeward_x(g):
        for o in (2 * g, 2 * g + 1):
            if o:
                arrive(("r", o), recv_r.at[o])
        v = recv_r[2 * g:2 * g + 2].reshape(128, 1024)
        p = jnp.dot(homeward, v, preferred_element_type=f32)
        send_x[g] = p.astype(bf).reshape(8, 16, 1024)
        for o in (4, 5, 2, 3, 6, 7, 1):
            zz, xx, cc = plane[o]
            push(("b", o, g), send_x.at[g, xx * 2 + cc], recv_b.at[g, j], device(zz, xx, cc))
        recv_b[g, j] = send_x[g, j]

    permute(0)
    permute(1)
    on(0)
    permute(2)
    own(1)
    permute(3)
    on(1)
    loads["gate"].wait()
    loads["up"].wait()
    loads["last"].wait()
    for p in range(4):
        if p > 0:
            gather_on(p)
            hidden_on(p - 1)
        if p < 3:
            gather_own(p + 1)
        hidden(p)
        if p > 0:
            outputs(p - 1)
    hidden_on(3)
    homeward_x(0)
    outputs(3)
    homeward_x(1)
    homeward_x(2)
    homeward_x(3)
    for g in range(4):
        for o in plane_order:
            arrive(("b", o, g), recv_b.at[g, place_of(o)])

    v = recv_b[...].reshape(512, 1024)
    blended = (jnp.dot(blend[:, 0:512], v, preferred_element_type=f32)
               + jnp.dot(blend[:, 512:1024], v, preferred_element_type=f32))
    send_f[...] = blended.astype(bf).reshape(4, 32, 1024)
    for way, t in (("O", over), ("R", right), ("L", left)):
        push(("f", way), send_f.at[t], fin.at[y], way_y[way])
    fin[y] = send_f[y]
    for way, t in (("R", left), ("L", right), ("O", over)):
        arrive(("f", way), fin.at[t])
    square = jnp.zeros((32, 1), f32)
    for t in range(4):
        v = fin[t].astype(f32)
        square = square + jnp.sum(v * v, axis=1, keepdims=True)
    scale = lax.rsqrt(square * (1.0 / 4096) + 1e-6)
    for t in range(4):
        cols = slice(t * 1024, (t + 1) * 1024)
        out_ref[:, cols] = (stream_ref[:, cols].astype(f32) + fin[t].astype(f32) * scale * last_ref[:, cols]).astype(bf)
    for it in sends + down_copies + passed_on + copies + sent:
        it.wait_send()


def layer(*args):
    vm = pl.BlockSpec(memory_space=pltpu.VMEM)
    hbm = pl.BlockSpec(memory_space=pl.ANY)
    dma = pltpu.SemaphoreType.DMA
    bf, f32 = jnp.bfloat16, jnp.float32
    inputs = [((128, 512), bf), ((128, 128), bf), ((128, 128), bf)]
    late_inputs = [((32, 4096), bf), ((512, 4096), bf), ((1, 4096), f32), ((2, 128), jnp.int32), ((1, 128), f32),
                   ((4096, 256), bf), ((4096, 256), bf), ((1, 4096), f32)]
    sizes = [((32, 4096), bf), ((4, 8, 16, 1024), bf), ((4, 256, 1024), bf),
             ((2, 32, 128, 128), bf), ((2, 32, 128, 128), bf), ((512, 128), bf), ((KB, KB), bf), ((512, 128), f32),
             ((512, 128), f32), ((128, 512), bf), ((2, 128, 1024), bf), ((4, 2, 32, 2048), bf),
             ((2, 32, 2048), bf), ((2, 32, 2048), bf), ((2, 32, 2048), bf), ((2, 32, 2048), bf), ((4, 4, 128, 128), bf),
             ((4, 8, 16, 1024), bf), ((8, 16, 4096), bf), ((8, 4, 16, 4096), bf), ((4, 4, 128, 256), bf), ((8, 4, 16, 1024), bf),
             ((8, 4, 16, 1024), bf), ((4, 8, 16, 1024), bf), ((4, 8, 16, 1024), bf), ((128, 1024), bf), ((4, 32, 1024), bf),
             ((4, 32, 1024), bf), ((512, 128), f32)]
    return pl.pallas_call(
        layer_kernel, out_shape=jax.ShapeDtypeStruct((32, 4096), bf), in_specs=[hbm] * 13, out_specs=vm,
        scratch_shapes=[pltpu.VMEM(*n) for n in inputs] + [pltpu.SMEM((1, 4), f32)] + [pltpu.VMEM(*n) for n in late_inputs + sizes]
        + [dma((126,)), dma((126,)), dma((6,)), dma((6,)), dma((6,)), dma((6,)), dma((144,)), dma((144,)), dma((13,))],
        compiler_params=pltpu.CompilerParams(collective_id=0, has_side_effects=True, vmem_limit_bytes=60 * 1024 * 1024),
    )(*args)


def on_device(
    queries, keys, values, break_bias, residual, w_out, ffn_gain, pick_ids, pair_logit, w_gate, w_up, w_down, out_gain
):
    return layer(
        queries, keys, values, break_bias.reshape(1, 4), residual, w_out, ffn_gain.reshape(1, -1), pick_ids.T,
        pair_logit.reshape(1, -1), w_gate[0], w_up[0], w_down[0], out_gain.reshape(1, -1)
    )


def solution(mesh):
    placed = (
        P("sp", "tp"),
        P("sp", "tp"),
        P("sp", "tp"),
        P("tp"),
        P(("sp", "tp"), None),
        P("tp", None),
        P(),
        P("sp", None),
        P("sp"),
        P("sp", None, "tp"),
        P("sp", None, "tp"),
        P("sp", "tp", None),
        P(),
    )
    return jax.shard_map(
        on_device, mesh=mesh, in_specs=placed, out_specs=P(("sp", "tp"), None), check_vma=False
    )
```
